512 devices in a mesh: sp: 128 (over z, y, core), tp: 4 (over x).
Axes of the slice: x: 4, y: 8, z: 8, core: 2. Of those that a mesh axis runs over, the one named last changes fastest.
Arguments:
- tokens: bfloat16 [32768, 2048], P(('sp', 'tp')), may hold values from -16 to 16
- w_query: bfloat16 [2048, 1024], P(None, 'tp'), may hold values from -1 to 1
- w_key: bfloat16 [2048, 256], P(None, 'tp'), may hold values from -1 to 1
- w_value: bfloat16 [2048, 256], P(None, 'tp'), may hold values from -0.125 to 0.125
- w_gate: bfloat16 [2048, 16], P(None, 'tp'), may hold values from -0.125 to 0.125
- gate_bias: float32 [16], P('tp'), as said below
- w_output: bfloat16 [1024, 2048], P('tp'), may hold values from -0.1875 to 0.1875
Outputs:
- mixed: bfloat16 [32768, 2048], P(('sp', 'tp'))
The draws below stay inside these ranges and needn't reach their ends.
Inputs may be any that keep to these rules, and one draw needn't show every extreme that they name: `gate_bias`: each head's forget gate bias is 4 or more; there is no upper bound.
All inputs are finite; a program needn't handle non-finite values.
Results may differ from the reference program's by a relative error of at most 0.012.
The reference program's roundings to bfloat16 on the way count: a program that leaves them out, or rounds other values in their place, can miss the bound.
Values may be sent and summed in bfloat16 or wider, within the bound.
No kernel may reach another device: no remote copies, remote signals or barrier semaphores. Data moves between devices by JAX's collectives and lax.ppermute only.
A program may use at most 64 MiB of HBM per device.

```python
import math
import jax
import jax.numpy as jnp
from jax import lax

D = 2048
HEADS = 16
KV_HEADS = 4
HEAD = 64
TOK_DEV = 256
SEQ = 32768
N_TP = 4


def query_base(base_key):
    raw_values = jax.random.normal(jax.random.fold_in(base_key, 11), (D, HEADS * HEAD), jnp.float32)
    return jnp.clip(raw_values, -5.0, 5.0) / math.sqrt(D)


def draw_w_query(key, part):
    return query_base(key).astype(jnp.bfloat16)


def draw_w_key(key, part):
    raw_values = jax.random.normal(jax.random.fold_in(key, 12), (D, KV_HEADS * HEAD), jnp.float32)
    return (jnp.clip(raw_values, -5.0, 5.0) / math.sqrt(D)).astype(jnp.bfloat16)


def draw_gate_bias(key, part):
    shuffled = jax.random.permutation(jax.random.fold_in(key, 21), HEADS)
    quick = shuffled < HEADS // 2
    lasting = math.log(SEQ) + jax.random.uniform(jax.random.fold_in(key, 22), (HEADS,), jnp.float32, 0.5, 1.5)
    fading = jax.random.uniform(jax.random.fold_in(key, 23), (HEADS,), jnp.float32, 4.1, 5.3)
    return jnp.where(quick, fading, lasting).astype(jnp.float32)


def draw_tokens(key, part):
    span_rows = TOK_DEV // 2
    span_count = SEQ // span_rows
    scales = jnp.exp(jax.random.uniform(jax.random.fold_in(key, 31), (span_count, 1, 1), jnp.float32, math.log(0.6), math.log(1.6)))
    shifts = jax.random.uniform(jax.random.fold_in(key, 32), (span_count, 1, 1), jnp.float32, -1.5, 1.5)
    heading = jnp.clip(jax.random.normal(jax.random.fold_in(key, 33), (1, 1, D), jnp.float32), -3.0, 3.0)
    noise = jnp.clip(jax.random.normal(jax.random.fold_in(key, 34), (span_count, span_rows, D), jnp.float32), -5.0, 5.0)
    field = (scales * (noise + shifts * heading)).reshape(SEQ, D)
    return jnp.clip(field, -16.0, 16.0).astype(jnp.bfloat16)


def block_levels(stream_key, dims, pieces, low, largest):
    loudness = 1.0
    for axis_at, shards_of in pieces:
        steps = jax.random.uniform(jax.random.fold_in(jax.random.fold_in(stream_key, 6), axis_at), (shards_of,), jnp.float32, low / len(pieces), largest / len(pieces))
        loudness = loudness * jnp.repeat(jnp.exp(steps), dims[axis_at] // shards_of).reshape((-1,) + (1,) * (len(dims) - 1 - axis_at))
    return loudness


def normal_values(key, extent, deviation, reach, shards=(), kind=jnp.bfloat16):
    values = jax.random.normal(key, extent, jnp.float32) * deviation
    if len(shards) > 0:
        values = block_levels(key, extent, shards, -0.22, 0.18) * values
    return jnp.clip(values, min=-reach, max=reach).astype(kind)


def setup_inputs(seed: int = 0) -> dict:
    splits = jax.random.split(jax.random.key(seed), 8)
    return {
        "tokens": draw_tokens(jax.random.fold_in(splits[7], 71), 0),
        "w_query": draw_w_query(jax.random.fold_in(splits[7], 71), 0),
        "w_key": draw_w_key(jax.random.fold_in(splits[7], 71), 0),
        "w_value": normal_values(splits[3], (D, KV_HEADS * HEAD), D ** -0.5, 0.125, ((1, 4),)),
        "w_gate": normal_values(splits[4], (D, HEADS), D ** -0.5, 0.125, ((1, 4),)),
        "gate_bias": draw_gate_bias(jax.random.fold_in(splits[7], 71), 0),
        "w_output": normal_values(splits[6], (HEADS * HEAD, D), (HEADS * HEAD) ** -0.5, 0.1875, ((0, 4),)),
    }


masked_value = -1e30


def reference(tokens, w_query, w_key, w_value, w_gate, gate_bias, w_output):
    length = tokens.shape[0]
    group_size = HEADS // KV_HEADS
    queries = jnp.dot(tokens, w_query, preferred_element_type=jnp.float32).astype(jnp.bfloat16)
    key_proj = jnp.dot(tokens, w_key, preferred_element_type=jnp.float32).astype(jnp.bfloat16)
    value_proj = jnp.dot(tokens, w_value, preferred_element_type=jnp.float32).astype(jnp.bfloat16)
    gate_logits = jnp.dot(tokens, w_gate, preferred_element_type=jnp.float32).astype(jnp.bfloat16)
    queries, key_proj, value_proj, gate_logits = lax.optimization_barrier((queries, key_proj, value_proj, gate_logits))
    log_gates = jax.nn.log_sigmoid(gate_logits.astype(jnp.float32) + gate_bias.astype(jnp.float32))
    cumulative = jnp.cumsum(log_gates, axis=0)
    span = math.gcd(length, 512)
    block_total = length // span
    query_all = queries.astype(jnp.float32).reshape(block_total, span, KV_HEADS, group_size, HEAD)
    key_all = key_proj.astype(jnp.float32).reshape(block_total, span, KV_HEADS, HEAD)
    value_all = value_proj.astype(jnp.float32).reshape(block_total, span, KV_HEADS, HEAD)
    cumul_all = cumulative.reshape(block_total, span, KV_HEADS, group_size)
    scale = HEAD ** -0.5

    def query_block(block_index):
        query_here = lax.dynamic_index_in_dim(query_all, block_index, 0, keepdims=False)
        cumul_here = lax.dynamic_index_in_dim(cumul_all, block_index, 0, keepdims=False).transpose(1, 2, 0)
        query_position = block_index * span + jnp.arange(span, dtype=jnp.int32)

        def key_step(key_index, carry_state):
            row_peak, row_mass, row_accum = carry_state
            key_here = lax.dynamic_index_in_dim(key_all, key_index, 0, keepdims=False)
            value_here = lax.dynamic_index_in_dim(value_all, key_index, 0, keepdims=False)
            key_cumul = lax.dynamic_index_in_dim(cumul_all, key_index, 0, keepdims=False).transpose(1, 2, 0)
            key_position = key_index * span + jnp.arange(span, dtype=jnp.int32)
            scores = jnp.einsum("tkgd,skd->kgts", query_here, key_here) * scale
            scores = scores + cumul_here[:, :, :, None] - key_cumul[:, :, None, :]
            allowed = key_position[None, :] <= query_position[:, None]
            scores = jnp.where(allowed, scores, masked_value)
            new_peak = jnp.maximum(row_peak, jnp.max(scores, axis=3))
            weights = jnp.where(allowed, jnp.exp(scores - new_peak[:, :, :, None]), 0.0)
            rescale = jnp.exp(row_peak - new_peak)
            row_mass = row_mass * rescale + jnp.sum(weights, axis=3)
            weights_low = lax.optimization_barrier(weights.astype(jnp.bfloat16))
            row_accum = row_accum * rescale[:, :, :, None] + jnp.einsum(
                "kgts,skd->kgtd", weights_low.astype(jnp.float32), value_here)
            return new_peak, row_mass, row_accum

        initial = (jnp.full((KV_HEADS, group_size, span), masked_value, jnp.float32),
                   jnp.zeros((KV_HEADS, group_size, span), jnp.float32),
                   jnp.zeros((KV_HEADS, group_size, span, HEAD), jnp.float32))
        row_peak, row_mass, row_accum = lax.fori_loop(0, block_index + 1, key_step, initial)
        attended = (row_accum / row_mass[:, :, :, None]).astype(jnp.bfloat16)
        return attended.transpose(2, 0, 1, 3).reshape(span, HEADS * HEAD)

    attended = lax.map(query_block, jnp.arange(block_total, dtype=jnp.int32)).reshape(length, HEADS * HEAD)
    per_group = HEADS * HEAD // N_TP
    total = jnp.zeros((length, D), jnp.float32)
    for group_index in range(N_TP):
        partial_value = jnp.dot(attended[:, group_index * per_group:(group_index + 1) * per_group],
                          w_output[group_index * per_group:(group_index + 1) * per_group],
                          preferred_element_type=jnp.float32).astype(jnp.bfloat16)
        partial_value = lax.optimization_barrier(partial_value)
        total = total + partial_value.astype(jnp.float32)
    return total.astype(jnp.bfloat16)
```

```python
import functools
import jax, jax.numpy as jnp
from jax import lax
from jax.experimental import pallas as pl
from jax.experimental.pallas import tpu as pltpu
from jax.sharding import Mesh
from jax.sharding import PartitionSpec as P

f32, bf16 = jnp.float32, jnp.bfloat16
HEAD = 64
NEG = -1e30

def split3(x):
    a = x.astype(bf16).astype(f32)
    r = x - a
    b = r.astype(bf16).astype(f32)
    c = (r - b).astype(bf16).astype(f32)
    return a, b, c

def log_sigmoid(u):
    x = jnp.exp(-jnp.abs(u))
    series = x * (1 - x * (1 / 2 - x * (1 / 3 - x * (1 / 4 - x * (1 / 5 - x * (1 / 6 - x * (1 / 7)))))))
    return jnp.minimum(u, 0.0) - jnp.where(x < 0.0625, series, jnp.log(1 + x))

def dot(a, b):
    return jnp.dot(a, b, preferred_element_type=f32)

def attend_kernel(info, kv, q, bias, acc_out, ml_out, cum, aug, rhs, acc, ml, *, chips, blk):
    core, low, high, low_side = info[0], info[1], info[2], info[3]
    rows = chips * 8
    gates = kv[:, 128:136, :].astype(f32) + bias[...][None, :, :1]
    logs = log_sigmoid(gates).reshape(rows, blk)
    tri = (lax.broadcasted_iota(jnp.int32, (blk, blk), 0) <= lax.broadcasted_iota(jnp.int32, (blk, blk), 1)).astype(bf16)
    inner = sum(dot(p.astype(bf16), tri) for p in split3(logs))
    r0 = lax.broadcasted_iota(jnp.int32, (rows, rows), 0)
    r1 = lax.broadcasted_iota(jnp.int32, (rows, rows), 1)
    before = ((r1 < r0) & (((r0 - r1) & 3) == 0)).astype(bf16)
    last = jnp.broadcast_to(inner[:, blk - 1:], (rows, blk))
    outer = sum(dot(before, p.astype(bf16)) for p in split3(last))
    total = (inner + outer).reshape(chips, 8, blk)
    cum[...] = total
    own = jnp.where(core == 0, total[:, :4], total[:, 4:])
    parts = split3(-own)
    ones = jnp.ones((chips, 4, blk), f32)
    aug[...] = jnp.concatenate([*parts, ones], axis=1).astype(bf16)
    row16 = lax.broadcasted_iota(jnp.int32, (16, blk), 0)
    for side in range(2):
        which = low_side if side == 0 else 1 - low_side
        chip = low if side == 0 else high
        here = cum[chip]
        here = jnp.where(which == 0, here[:4], here[4:])
        pa, pb, pc = split3(here)
        for h in range(4):
            tail = jnp.where((row16 < 12) & ((row16 & 3) == h), 1.0, 0.0)
            tail = jnp.where(row16 == 12, pa[h:h + 1], tail)
            tail = jnp.where(row16 == 13, pb[h:h + 1], tail)
            tail = jnp.where(row16 == 14, pc[h:h + 1], tail)
            qh = q[which, h * HEAD:(h + 1) * HEAD, :].astype(f32) * 0.125
            rhs[side * 4 + h] = jnp.concatenate([qh, tail, jnp.zeros((48, blk), f32)], axis=0).astype(bf16)
    acc[...] = jnp.zeros_like(acc)
    ml[0:8] = jnp.full((8, blk), NEG, f32)
    ml[8:16] = jnp.zeros((8, blk), f32)
    zeros = jnp.zeros((48, blk), bf16)

    def tile(jj, sides):
        lhs, vals = [], []
        for e in range(2):
            j = 2 * jj + e
            lhs.append(jnp.concatenate([kv[j, 0:64, :], aug[j], zeros], axis=0).T)
            vals.append(kv[j, 64:128, :])
        keys = jnp.concatenate(lhs, axis=0)
        for side, masked in sides:
            if masked:
                which = low_side if side == 0 else 1 - low_side
                chip = low if side == 0 else high
                qpos = (2 * chip + which) * blk + lax.broadcasted_iota(jnp.int32, (2 * blk, blk), 1)
                row = lax.broadcasted_iota(jnp.int32, (2 * blk, blk), 0)
                kpos = row + (row // blk) * blk + (4 * jj + core) * blk
                allowed = kpos <= qpos
            for h in range(4):
                u = side * 4 + h
                s = dot(keys, rhs[u])
                if masked:
                    s = jnp.where(allowed, s, NEG)
                m_old = ml[u:u + 1]
                m_new = jnp.maximum(m_old, jnp.max(s, axis=0, keepdims=True))
                p = jnp.exp(s - m_new)
                if masked:
                    p = jnp.where(allowed, p, 0.0)
                scale = jnp.exp(m_old - m_new)
                ml[u:u + 1] = m_new
                ml[8 + u:9 + u] = ml[8 + u:9 + u] * scale + jnp.sum(p, axis=0, keepdims=True)
                pb = p.astype(bf16)
                out = dot(vals[0], pb[:blk]) + dot(vals[1], pb[blk:])
                acc[u * HEAD:(u + 1) * HEAD] = acc[u * HEAD:(u + 1) * HEAD] * scale + out

    def both(jj, _):
        tile(jj, ((0, False), (1, False)))
        return _

    def one(jj, _):
        tile(jj, ((1, False),))
        return _

    lax.fori_loop(0, low // 2, both, 0)
    tile(low // 2, ((0, True), (1, False)))
    lax.fori_loop(low // 2 + 1, high // 2, one, 0)
    tile(high // 2, ((1, True),))
    for side in range(2):
        which = low_side if side == 0 else 1 - low_side
        acc_out[which] = acc[side * 256:(side + 1) * 256]
        ml_out[which] = jnp.concatenate([ml[side * 4:side * 4 + 4], ml[8 + side * 4:12 + side * 4]], axis=0)

def attend(info, kv, q, bias8, interpret=False):
    chips, _, blk = kv.shape
    vm = pl.BlockSpec(memory_space=pltpu.VMEM)
    return pl.pallas_call(
        functools.partial(attend_kernel, chips=chips, blk=blk),
        out_shape=(jax.ShapeDtypeStruct((2, 256, blk), f32), jax.ShapeDtypeStruct((2, 8, blk), f32)),
        in_specs=[pl.BlockSpec(memory_space=pltpu.SMEM), vm, vm, vm],
        out_specs=(vm, vm),
        scratch_shapes=[pltpu.VMEM((chips, 8, blk), f32), pltpu.VMEM((chips, 16, blk), bf16),
                        pltpu.VMEM((8, 128, blk), bf16), pltpu.VMEM((512, blk), f32), pltpu.VMEM((16, blk), f32)],
        compiler_params=pltpu.CompilerParams(vmem_limit_bytes=48 * 1024 * 1024),
        interpret=interpret, name='attend',
    )(info, kv, q, bias8)


SP = ("sp_0", "sp_1", "sp_2")
SP_TP = ("sp_0", "sp_1", "sp_2", "tp")


def sum_at_owner(value):
    pieces = value.reshape(4, value.shape[0] // 4, value.shape[1])
    arrived = lax.all_to_all(pieces, "tp", split_axis=0, concat_axis=0, tiled=True)
    return arrived.astype(f32).sum(axis=0)


def shards(tokens, w_query, w_key, w_value, w_gate, gate_bias, w_output):
    rows, cols = lax.axis_size("sp_0"), lax.axis_size("sp_1")
    chips = rows * cols
    core = lax.axis_index("sp_2")
    chip = lax.axis_index("sp_0") * cols + lax.axis_index("sp_1")
    other = chips - 1 - chip
    copies = jnp.broadcast_to(tokens, (4, *tokens.shape))
    here = lax.all_to_all(copies, "tp", split_axis=0, concat_axis=0, tiled=True)
    here = here.reshape(-1, tokens.shape[1])
    joined = jnp.concatenate([w_query, w_key, w_value, w_gate], axis=1)
    projected = lax.dot_general(joined, here, (((0,), (1,)), ((), ())), preferred_element_type=f32).astype(bf16)
    query = projected[:256]
    gates = projected[384:388]
    swapped = lax.ppermute(gates, "sp_2", [(0, 1), (1, 0)])
    first = jnp.where(core == 0, gates, swapped)
    second = jnp.where(core == 0, swapped, gates)
    payload = jnp.concatenate([projected[256:384], first, second], axis=0)
    blk = payload.shape[1]
    spread = jnp.broadcast_to(payload, (cols, *payload.shape))
    row = lax.all_to_all(spread, "sp_1", split_axis=0, concat_axis=0, tiled=True)
    kv = lax.all_gather(row, "sp_0").reshape(chips, 136, blk)
    moves = []
    for c in range(chips):
        moves.append((2 * c, 2 * c + 1))
        moves.append((2 * c + 1, 2 * (chips - 1 - c)))
    arrived = lax.ppermute(query, SP, moves)
    far = [(2 * c + 1, 2 * (chips - 1 - c) + 1) for c in range(chips)]
    crossed = lax.ppermute(query, SP, far)
    q = jnp.stack([jnp.where(core == 0, query, arrived), jnp.where(core == 0, arrived, crossed)])
    info = jnp.stack([core, jnp.minimum(chip, other), jnp.maximum(chip, other), (chip > other).astype(jnp.int32)])
    bias8 = jnp.broadcast_to(jnp.tile(gate_bias, 2)[:, None], (8, 128))
    acc, ml = attend(info.astype(jnp.int32), kv, q, bias8)
    state = jnp.concatenate([acc, ml], axis=1)
    give = lax.dynamic_index_in_dim(state, 1 - core, 0, keepdims=False)
    keep = lax.dynamic_index_in_dim(state, core, 0, keepdims=False)
    got = lax.ppermute(give, "sp_2", [(0, 1), (1, 0)])
    peak = jnp.maximum(keep[256:260], got[256:260])
    wa, wb = jnp.exp(keep[256:260] - peak), jnp.exp(got[256:260] - peak)
    mass = keep[260:264] * wa + got[260:264] * wb
    accum = keep[:256].reshape(4, 64, blk) * wa[:, None] + got[:256].reshape(4, 64, blk) * wb[:, None]
    attended = (accum / mass[:, None]).astype(bf16).reshape(256, blk)
    returned = lax.ppermute(attended, SP, far)
    attended = jnp.where(core == 0, attended, returned)
    partial = lax.dot_general(attended, w_output, (((0,), (0,)), ((), ())), preferred_element_type=f32).astype(bf16)
    return sum_at_owner(partial).astype(bf16)


def solution(mesh):
    finer = Mesh(mesh.devices.reshape(8, 8, 2, mesh.shape["tp"]), SP_TP)
    placed = (P(SP_TP, None), P(None, "tp"), P(None, "tp"), P(None, "tp"), P(None, "tp"), P("tp"), P("tp", None))
    return jax.shard_map(shards, mesh=finer, in_specs=placed, out_specs=P(SP_TP, None), check_vma=False)
```

```python
import functools
import jax, jax.numpy as jnp
from jax import lax
from jax.experimental import pallas as pl
from jax.experimental.pallas import tpu as pltpu
from jax.sharding import Mesh
from jax.sharding import PartitionSpec as P

f32, bf16 = jnp.float32, jnp.bfloat16
HEAD = 64
NEG = -1e30
LOW = -1e20

def split3(x):
    a = x.astype(bf16).astype(f32)
    r = x - a
    b = r.astype(bf16).astype(f32)
    return a, b, r - b

def log_sigmoid(u):
    x = jnp.exp(-jnp.abs(u))
    series = x * (1 - x * (1 / 2 - x * (1 / 3 - x * (1 / 4 - x * (1 / 5 - x * (1 / 6 - x * (1 / 7)))))))
    return jnp.minimum(u, 0.0) - jnp.where(x < 0.0625, series, jnp.log(1 + x))

def dot(a, b):
    return jnp.dot(a, b, preferred_element_type=f32)

def attend_kernel(*refs, count, chips, blk):
    info, q, bias = refs[:3]
    kvs = refs[3:3 + count]
    acc, stat, tot = refs[3 + count:6 + count]
    aug, rhs, keys, scores, tops = refs[6 + count:]
    core = info[0]
    rows = chips * 8
    tri = (lax.broadcasted_iota(jnp.int32, (blk, blk), 0) <= lax.broadcasted_iota(jnp.int32, (blk, blk), 1)).astype(bf16)
    r0 = lax.broadcasted_iota(jnp.int32, (rows, rows), 0)
    r1 = lax.broadcasted_iota(jnp.int32, (rows, rows), 1)
    before = ((r1 < r0) & (((r0 - r1) & 3) == 0)).astype(bf16)
    row16 = lax.broadcasted_iota(jnp.int32, (16, blk), 0)
    for side in range(2):
        for h in range(4):
            mark = jnp.where((row16 < 12) & ((row16 & 3) == h), 1.0, 0.0).astype(bf16)
            qh = q[side, h * HEAD:(h + 1) * HEAD, :] * jnp.asarray(0.125, bf16)
            rhs[side * 4 + h] = jnp.concatenate([qh, mark, jnp.zeros((48, blk), bf16)], axis=0)
    zeros = jnp.zeros((48, blk), bf16)
    for n in range(count):
        kv = kvs[n]
        gates = kv[:, 128:136, :].astype(f32) + bias[...][None, :, :1]
        logs = log_sigmoid(gates).reshape(rows, blk)
        inner = sum(dot(p.astype(bf16), tri) for p in split3(logs))
        last = jnp.broadcast_to(inner[:, blk - 1:], (rows, blk))
        outer = sum(dot(before, p.astype(bf16)) for p in split3(last))
        total = (inner + outer).reshape(chips, 8, blk)
        own = jnp.where(core == 0, total[:, :4], total[:, 4:])
        tot[n] = jnp.broadcast_to(total[chips - 1][:, blk - 1:], (8, 128))
        aug[...] = jnp.concatenate([*split3(-own), jnp.zeros((chips, 4, blk), f32)], axis=1).astype(bf16)
        acc[n] = jnp.zeros((2, 256, blk), f32)
        for side in range(2):
            stat[n, side, 0:32] = jnp.zeros((32, blk), f32)
            stat[n, side, 32:64] = jnp.full((32, blk), LOW, f32)
        first = info[3 + n] * chips
        rel = [info[1] - first, info[2] - first]
        full = [jnp.clip(x, 0, chips) // 2 for x in rel]
        steps = full[0] + full[1]

        def place(it):
            side = (it >= full[0]).astype(jnp.int32)
            return side, jnp.minimum(it - side * full[0], chips // 2 - 1)

        def load_keys(slot, jj):
            for e in range(2):
                keys[slot, e * blk:(e + 1) * blk] = jnp.concatenate([kv[2 * jj + e, 0:64, :], aug[2 * jj + e], zeros], axis=0).T

        def score(slot, key_slot, side, h, allowed=None):
            s = dot(keys[key_slot], rhs[side * 4 + h])
            if allowed is not None:
                s = jnp.where(allowed, s, NEG)
            scores[slot] = s
            tops[slot] = jnp.max(s.reshape(2 * blk // 8, 8, blk), axis=0)

        def soften(slot, jj, side, h):
            old = stat[n, side, 32 + 8 * h:40 + 8 * h]
            new = jnp.maximum(old, jnp.max(tops[slot], axis=0, keepdims=True))
            scale = jnp.exp(old - new)
            mass = stat[n, side, 8 * h:8 * h + 8] * scale
            out = jnp.zeros((64, blk), f32)
            for e in range(2):
                s = scores[slot, e * blk:(e + 1) * blk].reshape(blk // 8, 8, blk)
                p = jnp.exp(s - new[None])
                mass = mass + jnp.sum(p, axis=0)
                out = out + dot(kv[2 * jj + e, 64:128, :], p.reshape(blk, blk).astype(bf16))
            stat[n, side, 8 * h:8 * h + 8] = mass
            stat[n, side, 32 + 8 * h:40 + 8 * h] = new
            a = acc[n, side, h * HEAD:(h + 1) * HEAD].reshape(8, 8, blk) * scale[None]
            acc[n, side, h * HEAD:(h + 1) * HEAD] = a.reshape(64, blk) + out

        @pl.when(steps > 0)
        def _():
            side, jj = place(0)
            load_keys(0, jj)
            score(0, 0, side, 0)

            def body(it, carry):
                slot = it & 1
                side, jj = place(it)
                side_next, jj_next = place(jnp.minimum(it + 1, steps - 1))
                load_keys(1 - slot, jj_next)
                for h in range(4):
                    if h < 3:
                        score((h + 1) & 1, slot, side, h + 1)
                    else:
                        score(0, 1 - slot, side_next, 0)
                    soften(h & 1, jj, side, h)
                return carry

            lax.fori_loop(0, steps, body, 0)

        def edge(side, carry):
            where = jnp.where(side == 0, rel[0], rel[1])

            @pl.when((where >= 0) & (where < chips))
            def _():
                jj = jnp.clip(where, 0, chips - 1) // 2
                par = jnp.where(side == 0, info[7], 1 - info[7])
                qpos = (2 * where + par) * blk + lax.broadcasted_iota(jnp.int32, (2 * blk, blk), 1)
                row = lax.broadcasted_iota(jnp.int32, (2 * blk, blk), 0)
                kpos = row + (row // blk) * blk + (4 * jj + core) * blk
                allowed = kpos <= qpos
                load_keys(0, jj)
                score(0, 0, side, 0, allowed)
                for h in range(4):
                    if h < 3:
                        score((h + 1) & 1, 0, side, h + 1, allowed)
                    soften(h & 1, jj, side, h)

            return carry

        lax.fori_loop(0, 2, edge, 0)

def attend_chunks(info, q, bias8, kvs):
    count = len(kvs)
    chips, _, blk = kvs[0].shape
    vm = pl.BlockSpec(memory_space=pltpu.VMEM)
    return pl.pallas_call(
        functools.partial(attend_kernel, count=count, chips=chips, blk=blk),
        out_shape=(jax.ShapeDtypeStruct((count, 2, 256, blk), f32), jax.ShapeDtypeStruct((count, 2, 64, blk), f32),
                   jax.ShapeDtypeStruct((count, 8, 128), f32)),
        in_specs=[pl.BlockSpec(memory_space=pltpu.SMEM), vm, vm] + [vm] * count,
        out_specs=(vm, vm, vm),
        scratch_shapes=[pltpu.VMEM((chips, 16, blk), bf16), pltpu.VMEM((8, 128, blk), bf16),
                        pltpu.VMEM((2, 2 * blk, 128), bf16), pltpu.VMEM((2, 2 * blk, blk), f32), pltpu.VMEM((2, 8, blk), f32)],
        compiler_params=pltpu.CompilerParams(vmem_limit_bytes=32 * 1024 * 1024),
    )(info, q, bias8, *kvs)

def merge_kernel(*refs, counts):
    info = refs[0]
    k = len(counts)
    accs, stats, tots = refs[1:1 + k], refs[1 + k:1 + 2 * k], refs[1 + 2 * k:1 + 3 * k]
    keep, give = refs[1 + 3 * k:]
    flat = [(i, n) for i in range(k) for n in range(counts[i])]
    rows = [info[2 + j] for j in range(len(flat))]
    base = []
    for j in range(len(flat)):
        b = jnp.zeros((4, 128), f32)
        for j2, (i2, n2) in enumerate(flat):
            if j2 != j:
                b = b + jnp.where(rows[j2] < rows[j], tots[i2][n2, 4:8], 0.0)
        base.append(b[:, :1])
    for which in range(2):
        dst = keep if which == 0 else give
        side = info[which]
        for h in range(4):
            tops = [stats[i][n, side, 32 + 8 * h:40 + 8 * h] - base[j][h:h + 1] for j, (i, n) in enumerate(flat)]
            top = functools.reduce(jnp.maximum, tops)
            w = [jnp.exp(t - top) for t in tops]
            mass = sum(stats[i][n, side, 8 * h:8 * h + 8] * w[j] for j, (i, n) in enumerate(flat))
            dst[256 + h:257 + h] = top[:1]
            dst[260 + h:261 + h] = jnp.sum(mass, axis=0, keepdims=True)
            tot = None
            for j, (i, n) in enumerate(flat):
                a = accs[i][n, side, h * HEAD:(h + 1) * HEAD].reshape(8, 8, 256) * w[j][None]
                tot = a if tot is None else tot + a
            dst[h * HEAD:(h + 1) * HEAD] = tot.reshape(HEAD, 256)

def merge(info, parts):
    counts = [p[0].shape[0] for p in parts]
    vm = pl.BlockSpec(memory_space=pltpu.VMEM)
    shape = jax.ShapeDtypeStruct((264, 256), f32)
    return pl.pallas_call(
        functools.partial(merge_kernel, counts=counts), out_shape=(shape, shape),
        in_specs=[pl.BlockSpec(memory_space=pltpu.SMEM)] + [vm] * (3 * len(parts)), out_specs=(vm, vm),
        compiler_params=pltpu.CompilerParams(vmem_limit_bytes=32 * 1024 * 1024), name='merge',
    )(info, *[p[0] for p in parts], *[p[1] for p in parts], *[p[2] for p in parts])

def finish_kernel(keep, got, out):
    peak = jnp.maximum(keep[256:260], got[256:260])
    wa, wb = jnp.exp(keep[256:260] - peak), jnp.exp(got[256:260] - peak)
    mass = keep[260:264] * wa + got[260:264] * wb
    for h in range(4):
        s = slice(h * HEAD, (h + 1) * HEAD)
        out[s] = ((keep[s] * wa[h:h + 1] + got[s] * wb[h:h + 1]) / mass[h:h + 1]).astype(bf16)

def finish(keep, got):
    vm = pl.BlockSpec(memory_space=pltpu.VMEM)
    return pl.pallas_call(finish_kernel, out_shape=jax.ShapeDtypeStruct((256, 256), bf16), in_specs=[vm, vm], out_specs=vm,
                          name='finish')(keep, got)


SP = ("sp_0", "sp_1", "sp_2")
SP_TP = ("sp_0", "sp_1", "sp_2", "tp")


def ring(count, step):
    return [(i, (i + step) % count) for i in range(count)]


def sum_at_owner(value):
    pieces = value.reshape(4, value.shape[0] // 4, value.shape[1])
    arrived = lax.all_to_all(pieces, "tp", split_axis=0, concat_axis=0, tiled=True)
    return arrived.astype(f32).sum(axis=0)


def shards(tokens, w_query, w_key, w_value, w_gate, gate_bias, w_output):
    rows, cols = lax.axis_size("sp_0"), lax.axis_size("sp_1")
    chips = rows * cols
    core = lax.axis_index("sp_2")
    row = lax.axis_index("sp_0")
    chip = row * cols + lax.axis_index("sp_1")
    other = chips - 1 - chip
    copies = jnp.broadcast_to(tokens, (4, *tokens.shape))
    here = lax.all_to_all(copies, "tp", split_axis=0, concat_axis=0, tiled=True)
    here = here.reshape(-1, tokens.shape[1])
    joined = jnp.concatenate([w_query, w_gate, w_key, w_value], axis=1)
    projected = lax.dot_general(joined, here, (((0,), (1,)), ((), ())), preferred_element_type=f32).astype(bf16)
    query, gates = projected[:256], projected[256:260]
    swapped = lax.ppermute(projected[:260], "sp_2", [(0, 1), (1, 0)])
    first = jnp.where(core == 0, gates, swapped[256:])
    second = jnp.where(core == 0, swapped[256:], gates)
    payload = jnp.concatenate([projected[260:], first, second], axis=0)
    even = jnp.where(core == 0, query, swapped[:256])
    odd = jnp.where(core == 0, swapped[:256], query)
    far = [(2 * c + e, 2 * (chips - 1 - c) + e) for c in range(chips) for e in range(2)]
    crossed = lax.ppermute(odd, SP, far)
    spread = jnp.broadcast_to(payload, (cols, *payload.shape))
    own = lax.all_to_all(spread, "sp_1", split_axis=0, concat_axis=0, tiled=True)
    own, crossed = lax.optimization_barrier((own, crossed))
    behind = chip > other
    q = jnp.stack([jnp.where(behind, crossed, even), jnp.where(behind, even, crossed)])
    bias8 = jnp.broadcast_to(jnp.tile(gate_bias, 2)[:, None], (8, 128))
    low, high = jnp.minimum(chip, other), jnp.maximum(chip, other)
    low_core = behind.astype(jnp.int32)

    def run(chunks, at):
        at = (list(at) + [jnp.int32(0)] * 4)[:4]
        info = jnp.stack([core, low, high, *at, low_core]).astype(jnp.int32)
        return attend_chunks(info, q, bias8, chunks)

    parts, order = [], []
    up, down = own, own
    pending, where = [own], [row]
    for step in range(1, rows // 2 + 1):
        up = lax.ppermute(up, "sp_0", ring(rows, 1))
        following, places = [up], [(row - step) % rows]
        if 2 * step < rows:
            down = lax.ppermute(down, "sp_0", ring(rows, -1))
            following.append(down)
            places.append((row + step) % rows)
        parts.append(run(pending, where))
        order += where
        pending, where = following, places
    parts.append(run(pending, where))
    order += where
    mine = jnp.where(behind, 1 - core, core)
    keep, give = merge(jnp.stack([mine, 1 - mine, *order]).astype(jnp.int32), parts)
    got = lax.ppermute(give, "sp_2", [(0, 1), (1, 0)])
    attended = finish(keep, got)
    back = [(2 * c + 1, 2 * (chips - 1 - c) + 1) for c in range(chips)]
    returned = lax.ppermute(attended, SP, back)
    attended = jnp.where(core == 0, attended, returned)
    partial = lax.dot_general(attended, w_output, (((0,), (0,)), ((), ())), preferred_element_type=f32).astype(bf16)
    return sum_at_owner(partial).astype(bf16)


def solution(mesh):
    finer = Mesh(mesh.devices.reshape(8, 8, 2, mesh.shape["tp"]), SP_TP)
    placed = (P(SP_TP, None), P(None, "tp"), P(None, "tp"), P(None, "tp"), P(None, "tp"), P("tp"), P("tp", None))

    return jax.shard_map(shards, mesh=finer, in_specs=placed, out_specs=P(SP_TP, None), check_vma=False)
```

```python
import functools
import jax, jax.numpy as jnp
from jax import lax
from jax.experimental import pallas as pl
from jax.experimental.pallas import tpu as pltpu
from jax.sharding import Mesh
from jax.sharding import PartitionSpec as P

f32, bf16 = jnp.float32, jnp.bfloat16
HEAD = 64
NEG = -1e30
LOW = -1e20
PIECES = 4


def split3(x):
    a = x.astype(bf16).astype(f32)
    r = x - a
    b = r.astype(bf16).astype(f32)
    return a, b, r - b


def log_sigmoid(u):
    x = jnp.exp(-jnp.abs(u))
    series = x * (1 - x * (1 / 2 - x * (1 / 3 - x * (1 / 4 - x * (1 / 5 - x * (1 / 6 - x * (1 / 7)))))))
    return jnp.minimum(u, 0.0) - jnp.where(x < 0.0625, series, jnp.log(1 + x))


def dot(a, b):
    return jnp.dot(a, b, preferred_element_type=f32)


def vmem(count):
    return [pl.BlockSpec(memory_space=pltpu.VMEM)] * count


def scalars():
    return pl.BlockSpec(memory_space=pltpu.SMEM)


def pack_kernel(info, mine, theirs, bias, payload, total, even, odd):
    first = info[0] == 0
    own, other = mine[256:260].astype(f32), theirs[256:260].astype(f32)
    gates = jnp.concatenate([jnp.where(first, own, other), jnp.where(first, other, own)], axis=0)
    payload[0:128] = mine[260:388]
    payload[128:136] = gates.astype(bf16)
    logs = jnp.sum(log_sigmoid(gates + bias[:, :1]), axis=1, keepdims=True)
    both = logs[:4] + logs[4:]
    total[...] = jnp.broadcast_to(jnp.concatenate([both, both], axis=0), total.shape)

    @pl.when(first)
    def _():
        even[...] = mine[0:256]
        odd[...] = theirs[0:256]

    @pl.when(jnp.logical_not(first))
    def _():
        even[...] = theirs[0:256]
        odd[...] = mine[0:256]


def pack(info, mine, theirs, bias8):
    blk = mine.shape[1]
    return pl.pallas_call(
        pack_kernel,
        out_shape=(jax.ShapeDtypeStruct((136, blk), bf16), jax.ShapeDtypeStruct((8, 128), f32),
                   jax.ShapeDtypeStruct((256, blk), bf16), jax.ShapeDtypeStruct((256, blk), bf16)),
        in_specs=[scalars(), *vmem(3)], out_specs=tuple(vmem(4)), name="pack",
    )(info, mine, theirs, bias8)


def prepare_kernel(info, column, totals, even, crossed, bias, chunk, rhs, *, rows, cols, blk):
    core, col = info[0], info[1]
    n = rows * 8
    gates = column[:, 128:136, :].astype(f32) + bias[...][None, :, :1]
    logs = log_sigmoid(gates).reshape(n, blk)
    tri = (lax.broadcasted_iota(jnp.int32, (blk, blk), 0) <= lax.broadcasted_iota(jnp.int32, (blk, blk), 1)).astype(bf16)
    inner = sum(dot(p.astype(bf16), tri) for p in split3(logs)).reshape(rows, 8, blk)
    index = lax.broadcasted_iota(jnp.int32, (rows * cols, 8, 128), 0)
    values = totals[...]
    for i in range(rows):
        base = jnp.sum(jnp.where(index < cols * i + col, values, 0.0), axis=0)[:4, :1]
        here = inner[i]
        own = jnp.where(core == 0, here[:4], here[4:] + here[:4, blk - 1:]) + base
        chunk[i, 64:80] = jnp.concatenate([*split3(-own), jnp.zeros((4, blk), f32)], axis=0).astype(bf16)
        chunk[i, 0:64] = column[i, 0:64, :]
        chunk[i, 80:144] = column[i, 64:128, :]
    row16 = lax.broadcasted_iota(jnp.int32, (16, blk), 0)
    swap = info[2] == 1
    for side in range(2):
        for h in range(4):
            s = slice(h * HEAD, (h + 1) * HEAD)
            a, b = even[s].astype(f32), crossed[s].astype(f32)
            q = jnp.where(swap, b, a) if side == 0 else jnp.where(swap, a, b)
            mark = jnp.where((row16 < 12) & ((row16 & 3) == h), 1.0, 0.0)
            rhs[side * 4 + h] = jnp.concatenate([q * 0.125, mark, jnp.zeros((48, blk), f32)], axis=0).astype(bf16)


def prepare(info, column, totals, even, crossed, bias8, cols):
    rows, _, blk = column.shape
    return pl.pallas_call(
        functools.partial(prepare_kernel, rows=rows, cols=cols, blk=blk),
        out_shape=(jax.ShapeDtypeStruct((rows, 144, blk), bf16), jax.ShapeDtypeStruct((8, 128, blk), bf16)),
        in_specs=[scalars(), *vmem(5)], out_specs=tuple(vmem(2)), name="prepare",
    )(info, column, totals, even, crossed, bias8)


def attend_kernel(*refs, count, rows, cols, blk):
    info, rhs = refs[:2]
    chunks = refs[2:2 + count]
    acc, stat = refs[2 + count:4 + count]
    keys, scores, tops = refs[4 + count:]
    core = info[0]
    acc[...] = jnp.zeros_like(acc)
    for side in range(2):
        stat[side, 0:32] = jnp.zeros((32, blk), f32)
        stat[side, 32:64] = jnp.full((32, blk), LOW, f32)
    for n in range(count):
        kv = chunks[n]
        col = info[3 + n]
        ahead = [jnp.clip((info[1 + side] - col + cols - 1) // cols, 0, rows) for side in range(2)]
        full = [a // 2 for a in ahead]
        diag = [(info[1 + side] - col) % cols == 0 for side in range(2)]
        part = [diag[side] | (ahead[side] % 2 == 1) for side in range(2)]
        steps = full[0] + full[1]

        def place(it):
            side = (it >= full[0]).astype(jnp.int32)
            return side, jnp.clip(it - side * full[0], 0, rows // 2 - 1)

        def load_keys(slot, jj):
            for e in range(2):
                keys[slot, e * blk:(e + 1) * blk] = kv[2 * jj + e, 0:128, :].T

        def fused(nxt, cur, allowed=None):
            if cur is not None:
                slot, jj, side, h = cur
                old = stat[side, 32 + 8 * h:40 + 8 * h]
                new = jnp.maximum(old, jnp.max(tops[slot], axis=0, keepdims=True))
                scale = jnp.exp(old - new)
                mass = stat[side, 8 * h:8 * h + 8] * scale
                out = jnp.zeros((64, blk), f32)
            top = None
            size = blk // PIECES
            for e in range(2):
                ps = []
                for g in range(PIECES):
                    at = e * blk + g * size
                    if nxt is not None:
                        s = dot(keys[nxt[1], at:at + size], rhs[nxt[2] * 4 + nxt[3]])
                        if allowed is not None:
                            s = jnp.where(allowed[at:at + size], s, NEG)
                        scores[nxt[0], at:at + size] = s
                        t = jnp.max(s.reshape(size // 8, 8, blk), axis=0)
                        top = t if top is None else jnp.maximum(top, t)
                    if cur is not None:
                        p = jnp.exp(scores[slot, at:at + size].reshape(size // 8, 8, blk) - new[None])
                        mass = mass + jnp.sum(p, axis=0)
                        ps.append(p.reshape(size, blk).astype(bf16))
                if cur is not None:
                    out = out + dot(kv[2 * jj + e, 80:144, :], jnp.concatenate(ps, axis=0))
            if nxt is not None:
                tops[nxt[0]] = top
            if cur is not None:
                stat[side, 8 * h:8 * h + 8] = mass
                stat[side, 32 + 8 * h:40 + 8 * h] = new
                a = acc[side, h * HEAD:(h + 1) * HEAD].reshape(8, 8, blk) * scale[None]
                acc[side, h * HEAD:(h + 1) * HEAD] = a.reshape(64, blk) + out

        @pl.when(steps > 0)
        def _():
            side, jj = place(0)
            load_keys(0, jj)
            fused((0, 0, side, 0), None)

            def body(it, carry):
                slot = it & 1
                side, jj = place(it)
                side_next, jj_next = place(jnp.minimum(it + 1, steps - 1))
                load_keys(1 - slot, jj_next)
                for h in range(4):
                    nxt = ((h + 1) & 1, slot, side, h + 1) if h < 3 else (0, 1 - slot, side_next, 0)
                    fused(nxt, (h & 1, jj, side, h))
                return carry

            lax.fori_loop(0, steps, body, 0)

        def edge(side, carry):
            @pl.when(jnp.where(side == 0, part[0], part[1]))
            def _():
                chip = jnp.where(side == 0, info[1], info[2])
                jj = jnp.clip(jnp.where(side == 0, full[0], full[1]), 0, rows // 2 - 1)
                par = jnp.where(side == 0, info[5], 1 - info[5])
                qpos = (2 * chip + par) * blk + lax.broadcasted_iota(jnp.int32, (2 * blk, blk), 1)
                row = lax.broadcasted_iota(jnp.int32, (2 * blk, blk), 0)
                upper = (row >= blk).astype(jnp.int32)
                kpos = row + upper * ((2 * cols - 1) * blk) + ((2 * jj * cols + col) * 2 + core) * blk
                allowed = kpos <= qpos
                load_keys(0, jj)
                fused((0, 0, side, 0), None, allowed)
                for h in range(4):
                    fused(((h + 1) & 1, 0, side, h + 1) if h < 3 else None, (h & 1, jj, side, h), allowed)

            return carry

        lax.fori_loop(0, 2, edge, 0)


def attend(info, rhs, chunks, cols):
    rows, _, blk = chunks[0].shape
    return pl.pallas_call(
        functools.partial(attend_kernel, count=len(chunks), rows=rows, cols=cols, blk=blk),
        out_shape=(jax.ShapeDtypeStruct((2, 256, blk), f32), jax.ShapeDtypeStruct((2, 64, blk), f32)),
        in_specs=[scalars(), *vmem(1 + len(chunks))], out_specs=tuple(vmem(2)),
        scratch_shapes=[pltpu.VMEM((2, 2 * blk, 128), bf16), pltpu.VMEM((2, 2 * blk, blk), f32), pltpu.VMEM((2, 8, blk), f32)],
        compiler_params=pltpu.CompilerParams(vmem_limit_bytes=24 * 1024 * 1024), name="attend",
    )(info, rhs, *chunks)


def merge_kernel(*refs, count):
    info, accs, stats = refs[0], refs[1:1 + count], refs[1 + count:1 + 2 * count]
    keep, give = refs[1 + 2 * count:]
    for which in range(2):
        dst, side = (keep, give)[which], info[which]
        for h in range(4):
            tops = [s[side, 32 + 8 * h:40 + 8 * h] for s in stats]
            top = functools.reduce(jnp.maximum, tops)
            w = [jnp.exp(t - top) for t in tops]
            mass = sum(s[side, 8 * h:8 * h + 8] * w[j] for j, s in enumerate(stats))
            dst[256 + h:257 + h] = top[:1]
            dst[260 + h:261 + h] = jnp.sum(mass, axis=0, keepdims=True)
            parts = [a[side, h * HEAD:(h + 1) * HEAD].reshape(8, 8, 256) * w[j][None] for j, a in enumerate(accs)]
            dst[h * HEAD:(h + 1) * HEAD] = functools.reduce(jnp.add, parts).reshape(HEAD, 256)


def merge(info, parts):
    shape = jax.ShapeDtypeStruct((264, 256), f32)
    return pl.pallas_call(
        functools.partial(merge_kernel, count=len(parts)), out_shape=(shape, shape),
        in_specs=[scalars(), *vmem(2 * len(parts))], out_specs=tuple(vmem(2)), name="merge",
    )(info, *[p[0] for p in parts], *[p[1] for p in parts])


def finish_kernel(keep, got, out):
    peak = jnp.maximum(keep[256:260], got[256:260])
    wa, wb = jnp.exp(keep[256:260] - peak), jnp.exp(got[256:260] - peak)
    mass = keep[260:264] * wa + got[260:264] * wb
    for h in range(4):
        s = slice(h * HEAD, (h + 1) * HEAD)
        out[s] = ((keep[s] * wa[h:h + 1] + got[s] * wb[h:h + 1]) / mass[h:h + 1]).astype(bf16)


def finish(keep, got):
    return pl.pallas_call(finish_kernel, out_shape=jax.ShapeDtypeStruct((256, 256), bf16), in_specs=vmem(2), out_specs=vmem(1)[0],
                          name="finish")(keep, got)


SP = ("sp_0", "sp_1", "sp_2")
SP_TP = ("sp_0", "sp_1", "sp_2", "tp")


def ring(count, step):
    return [(i, (i + step) % count) for i in range(count)]


def sum_at_owner(value):
    pieces = value.reshape(4, value.shape[0] // 4, value.shape[1])
    arrived = lax.all_to_all(pieces, "tp", split_axis=0, concat_axis=0, tiled=True)
    return arrived.astype(f32).sum(axis=0)


def shards(tokens, w_query, w_key, w_value, w_gate, gate_bias, w_output):
    rows, cols = lax.axis_size("sp_0"), lax.axis_size("sp_1")
    chips = rows * cols
    core, col = lax.axis_index("sp_2"), lax.axis_index("sp_1")
    chip = lax.axis_index("sp_0") * cols + col
    other = chips - 1 - chip
    behind = (chip > other).astype(jnp.int32)
    low, high = jnp.minimum(chip, other), jnp.maximum(chip, other)
    bias8 = jnp.broadcast_to(jnp.tile(gate_bias, 2)[:, None], (8, 128))

    def scalar_row(*values):
        return jnp.stack([jnp.asarray(v, jnp.int32) for v in values])

    copies = jnp.broadcast_to(tokens, (4, *tokens.shape))
    here = lax.all_to_all(copies, "tp", split_axis=0, concat_axis=0, tiled=True)
    here = here.reshape(-1, tokens.shape[1])
    joined = jnp.concatenate([w_query, w_gate, w_key, w_value], axis=1)
    projected = lax.dot_general(joined, here, (((0,), (1,)), ((), ())), preferred_element_type=f32).astype(bf16)
    swapped = lax.ppermute(projected[:260], "sp_2", [(0, 1), (1, 0)])
    payload, total, even, odd = pack(scalar_row(core), projected, swapped, bias8)
    far = [(2 * c + e, 2 * (chips - 1 - c) + e) for c in range(chips) for e in range(2)]
    crossed = lax.ppermute(odd, SP, far)
    column = lax.all_to_all(jnp.broadcast_to(payload, (rows, *payload.shape)), "sp_0", split_axis=0, concat_axis=0, tiled=True)
    totals = lax.all_to_all(jnp.broadcast_to(total, (chips, *total.shape)), ("sp_0", "sp_1"), split_axis=0, concat_axis=0, tiled=True)
    own, rhs = prepare(scalar_row(core, col, behind), column, totals, even, crossed, bias8, cols)

    parts = []
    up, down = own, own
    pending, where = [own], [col]
    for step in range(1, cols // 2 + 1):
        up = lax.ppermute(up, "sp_1", ring(cols, 1))
        following, places = [up], [(col - step) % cols]
        if 2 * step < cols:
            down = lax.ppermute(down, "sp_1", ring(cols, -1))
            following.append(down)
            places.append((col + step) % cols)
        parts.append(attend(scalar_row(core, low, high, where[0], where[-1], behind), rhs, pending, cols))
        pending, where = following, places
    parts.append(attend(scalar_row(core, low, high, where[0], where[-1], behind), rhs, pending, cols))
    mine = jnp.where(behind == 1, 1 - core, core)
    keep, give = merge(scalar_row(mine, 1 - mine), parts)
    got = lax.ppermute(give, "sp_2", [(0, 1), (1, 0)])
    attended = finish(keep, got)
    back = [(2 * c + 1, 2 * (chips - 1 - c) + 1) for c in range(chips)]
    returned = lax.ppermute(attended, SP, back)
    attended = jnp.where(core == 0, attended, returned)
    partial = lax.dot_general(attended, w_output, (((0,), (0,)), ((), ())), preferred_element_type=f32).astype(bf16)
    return sum_at_owner(partial).astype(bf16)


def solution(mesh):
    finer = Mesh(mesh.devices.reshape(8, 8, 2, mesh.shape["tp"]), SP_TP)
    placed = (P(SP_TP, None), P(None, "tp"), P(None, "tp"), P(None, "tp"), P(None, "tp"), P("tp"), P("tp", None))

    return jax.shard_map(shards, mesh=finer, in_specs=placed, out_specs=P(SP_TP, None), check_vma=False)
```

```python
import functools
import jax, jax.numpy as jnp
from jax import lax
from jax.experimental import pallas as pl
from jax.experimental.pallas import tpu as pltpu
from jax.sharding import Mesh
from jax.sharding import PartitionSpec as P

f32, bf16 = jnp.float32, jnp.bfloat16
HEAD = 64
NEG = -1e30
LOW = -1e20
PIECES = 4
SMALL = pltpu.CompilerParams(vmem_limit_bytes=8 * 1024 * 1024)


def split3(x):
    a = x.astype(bf16).astype(f32)
    r = x - a
    b = r.astype(bf16).astype(f32)
    return a, b, r - b


def log_sigmoid(u):
    x = jnp.exp(-jnp.abs(u))
    series = x * (1 - x * (1 / 2 - x * (1 / 3 - x * (1 / 4 - x * (1 / 5 - x * (1 / 6 - x * (1 / 7)))))))
    return jnp.minimum(u, 0.0) - jnp.where(x < 0.0625, series, jnp.log(1 + x))


def dot(a, b):
    return jnp.dot(a, b, preferred_element_type=f32)


def vmem(count):
    return [pl.BlockSpec(memory_space=pltpu.VMEM)] * count


def scalars():
    return pl.BlockSpec(memory_space=pltpu.SMEM)


def sums_kernel(info, mine, theirs, bias, total, even, odd):
    first = info[0] == 0
    own, other = mine[256:260].astype(f32), theirs[256:260].astype(f32)
    gates = jnp.concatenate([jnp.where(first, own, other), jnp.where(first, other, own)], axis=0)
    logs = jnp.sum(log_sigmoid(gates + bias[:, :1]), axis=1, keepdims=True)
    both = logs[:4] + logs[4:]
    total[...] = jnp.broadcast_to(jnp.concatenate([both, logs[:4]], axis=0), total.shape)

    @pl.when(first)
    def _():
        even[...] = mine[0:256]
        odd[...] = theirs[0:256]

    @pl.when(jnp.logical_not(first))
    def _():
        even[...] = theirs[0:256]
        odd[...] = mine[0:256]


def sums(info, mine, theirs, bias8):
    blk = mine.shape[1]
    half = jax.ShapeDtypeStruct((256, blk), bf16)
    return pl.pallas_call(
        sums_kernel, out_shape=(jax.ShapeDtypeStruct((8, 128), f32), half, half),
        in_specs=[scalars(), *vmem(3)], out_specs=tuple(vmem(3)), compiler_params=SMALL, name="sums",
    )(info, mine, theirs, bias8)


def pack_kernel(mine, total, row, payload, *, cols):
    payload[0:128] = mine[260:388]
    lane = lax.broadcasted_iota(jnp.int32, (4, 128), 1)
    held = jnp.zeros((4, 128), f32)
    for j in range(cols + 1):
        values = row[j, 0:4] if j < cols else total[4:8]
        for p, part in enumerate(split3(values)):
            held = jnp.where(lane == 16 * p + j, part, held)
    held = jnp.concatenate([held, jnp.zeros((4, 128), f32)], axis=1)
    payload[128:136] = jnp.concatenate([mine[256:260].astype(f32), held], axis=0).astype(bf16)


def pack(mine, total, row):
    blk = mine.shape[1]
    return pl.pallas_call(
        functools.partial(pack_kernel, cols=row.shape[0]), out_shape=jax.ShapeDtypeStruct((136, blk), bf16),
        in_specs=vmem(3), out_specs=vmem(1)[0], compiler_params=SMALL, name="pack",
    )(mine, total, row)


def prepare_kernel(info, column, even, crossed, bias, chunk, rhs, *, rows, cols, blk):
    core, col = info[0], info[1]
    last = column[:, 128:136, :].astype(f32)
    logs = log_sigmoid(last + bias[...][None, :, :1]).reshape(rows * 8, blk)
    tri = (lax.broadcasted_iota(jnp.int32, (blk, blk), 0) <= lax.broadcasted_iota(jnp.int32, (blk, blk), 1)).astype(bf16)
    inner = sum(dot(p.astype(bf16), tri) for p in split3(logs)).reshape(rows, 8, blk)
    lane = lax.broadcasted_iota(jnp.int32, (rows, 8, blk), 2)
    which = lane & 15
    used = lane < 48
    whole = jnp.sum(jnp.where(used & (which < cols), last, 0.0), axis=2, keepdims=True)
    early = jnp.sum(jnp.where(used & ((which < col) | ((which == cols) & (core == 1))), last, 0.0), axis=2, keepdims=True)
    before = jnp.zeros((4, 1), f32)
    for i in range(rows):
        own = inner[i, :4] + (before + early[i, 4:])
        before = before + whole[i, 4:]
        chunk[i, 64:80] = jnp.concatenate([*split3(-own), jnp.zeros((4, blk), f32)], axis=0).astype(bf16)
        chunk[i, 0:64] = column[i, 0:64, :]
        chunk[i, 80:144] = column[i, 64:128, :]
    row16 = lax.broadcasted_iota(jnp.int32, (16, blk), 0)
    swap = info[2] == 1
    for side in range(2):
        for h in range(4):
            s = slice(h * HEAD, (h + 1) * HEAD)
            a, b = even[s].astype(f32), crossed[s].astype(f32)
            q = jnp.where(swap, b, a) if side == 0 else jnp.where(swap, a, b)
            mark = jnp.where((row16 == 12) | ((row16 < 12) & ((row16 & 3) == h)), 1.0, 0.0)
            rhs[side * 4 + h] = jnp.concatenate([q * 0.125, mark, jnp.zeros((48, blk), f32)], axis=0).astype(bf16)


def prepare(info, column, even, crossed, bias8, cols):
    rows, _, blk = column.shape
    return pl.pallas_call(
        functools.partial(prepare_kernel, rows=rows, cols=cols, blk=blk),
        out_shape=(jax.ShapeDtypeStruct((rows, 144, blk), bf16), jax.ShapeDtypeStruct((8, 128, blk), bf16)),
        in_specs=[scalars(), *vmem(4)], out_specs=tuple(vmem(2)), compiler_params=pltpu.CompilerParams(vmem_limit_bytes=16 * 1024 * 1024), name="prepare",
    )(info, column, even, crossed, bias8)


def attend_kernel(*refs, count, rows, cols, blk):
    info, rhs = refs[:2]
    chunks = refs[2:2 + count]
    acc, stat = refs[2 + count:4 + count]
    keys, scores, tops = refs[4 + count:]
    core = info[0]
    size = blk // PIECES
    row16 = lax.broadcasted_iota(jnp.int32, (16, blk), 0)
    acc[...] = jnp.zeros_like(acc)
    for side in range(2):
        stat[side, 0:32] = jnp.zeros((32, blk), f32)
        stat[side, 32:64] = jnp.full((32, blk), LOW, f32)
    for n in range(count):
        kv = chunks[n]
        col = info[3 + n]
        ahead = [jnp.clip((info[1 + side] - col + cols - 1) // cols, 0, rows) for side in range(2)]
        diag = [(info[1 + side] - col) % cols == 0 for side in range(2)]
        full = [jnp.where(diag[side], ahead[side], ahead[side] + 1) // 2 for side in range(2)]
        steps = full[0] + full[1]

        def place(it):
            side = (it >= full[0]).astype(jnp.int32)
            return side, jnp.clip(it - side * full[0], 0, rows // 2 - 1)

        def load_keys(slot, jj, count):
            for e in range(2):
                marks = kv[2 * jj + e, 64:80, :].astype(f32)
                marks = jnp.where((row16 == 12) & (2 * jj + e >= count), NEG, marks).astype(bf16)
                keys[slot, e * blk:(e + 1) * blk] = jnp.concatenate([kv[2 * jj + e, 0:64, :], marks, kv[2 * jj + e, 80:128, :]], axis=0).T

        def fused(nxt, cur, allowed=None):
            if cur is not None:
                slot, jj, side, h = cur
                old = stat[side, 32 + 8 * h:40 + 8 * h]
                new = jnp.maximum(old, jnp.max(tops[slot], axis=0, keepdims=True))
                scale = jnp.exp(old - new)
                mass = stat[side, 8 * h:8 * h + 8] * scale
                out = jnp.zeros((64, blk), f32)
            top = None
            for e in range(2):
                ps = []
                for g in range(PIECES):
                    at = e * blk + g * size
                    if nxt is not None:
                        s = dot(keys[nxt[1], at:at + size], rhs[nxt[2] * 4 + nxt[3]])
                        if allowed is not None:
                            s = jnp.where(allowed[at:at + size], s, NEG)
                        scores[nxt[0], at:at + size] = s
                        t = jnp.max(s.reshape(size // 8, 8, blk), axis=0)
                        top = t if top is None else jnp.maximum(top, t)
                    if cur is not None:
                        p = jnp.exp(scores[slot, at:at + size].reshape(size // 8, 8, blk) - new[None])
                        mass = mass + jnp.sum(p, axis=0)
                        ps.append(p.reshape(size, blk).astype(bf16))
                if cur is not None:
                    out = out + dot(kv[2 * jj + e, 80:144, :], jnp.concatenate(ps, axis=0))
            if nxt is not None:
                tops[nxt[0]] = top
            if cur is not None:
                stat[side, 8 * h:8 * h + 8] = mass
                stat[side, 32 + 8 * h:40 + 8 * h] = new
                a = acc[side, h * HEAD:(h + 1) * HEAD].reshape(8, 8, blk) * scale[None]
                acc[side, h * HEAD:(h + 1) * HEAD] = a.reshape(64, blk) + out

        @pl.when(steps > 0)
        def _():
            side, jj = place(0)
            load_keys(0, jj, jnp.where(side == 0, ahead[0], ahead[1]))
            fused((0, 0, side, 0), None)

            def body(it, carry):
                slot = it & 1
                side, jj = place(it)
                side_next, jj_next = place(jnp.minimum(it + 1, steps - 1))
                load_keys(1 - slot, jj_next, jnp.where(side_next == 0, ahead[0], ahead[1]))
                for h in range(4):
                    nxt = ((h + 1) & 1, slot, side, h + 1) if h < 3 else (0, 1 - slot, side_next, 0)
                    fused(nxt, (h & 1, jj, side, h))
                return carry

            lax.fori_loop(0, steps, body, 0)

        def edge(side, carry):
            @pl.when(jnp.where(side == 0, diag[0], diag[1]))
            def _():
                chip = jnp.where(side == 0, info[1], info[2])
                jj = jnp.clip(jnp.where(side == 0, full[0], full[1]), 0, rows // 2 - 1)
                par = jnp.where(side == 0, info[5], 1 - info[5])
                qpos = (2 * chip + par) * blk + lax.broadcasted_iota(jnp.int32, (2 * blk, blk), 1)
                row = lax.broadcasted_iota(jnp.int32, (2 * blk, blk), 0)
                upper = (row >= blk).astype(jnp.int32)
                kpos = row + upper * ((2 * cols - 1) * blk) + ((2 * jj * cols + col) * 2 + core) * blk
                allowed = kpos <= qpos
                load_keys(0, jj, rows)
                fused((0, 0, side, 0), None, allowed)
                for h in range(4):
                    fused(((h + 1) & 1, 0, side, h + 1) if h < 3 else None, (h & 1, jj, side, h), allowed)

            return carry

        lax.fori_loop(0, 2, edge, 0)


def attend(info, rhs, chunks, cols):
    rows, _, blk = chunks[0].shape
    return pl.pallas_call(
        functools.partial(attend_kernel, count=len(chunks), rows=rows, cols=cols, blk=blk),
        out_shape=(jax.ShapeDtypeStruct((2, 256, blk), f32), jax.ShapeDtypeStruct((2, 64, blk), f32)),
        in_specs=[scalars(), *vmem(1 + len(chunks))], out_specs=tuple(vmem(2)),
        scratch_shapes=[pltpu.VMEM((2, 2 * blk, 128), bf16), pltpu.VMEM((2, 2 * blk, blk), f32), pltpu.VMEM((2, 8, blk), f32)],
        compiler_params=pltpu.CompilerParams(vmem_limit_bytes=16 * 1024 * 1024), name="attend",
    )(info, rhs, *chunks)


def merge_kernel(*refs, count):
    info, accs, stats = refs[0], refs[1:1 + count], refs[1 + count:1 + 2 * count]
    keep, give = refs[1 + 2 * count:]
    for which in range(2):
        dst, side = (keep, give)[which], info[which]
        for h in range(4):
            tops = [s[side, 32 + 8 * h:40 + 8 * h] for s in stats]
            top = functools.reduce(jnp.maximum, tops)
            w = [jnp.exp(t - top) for t in tops]
            mass = sum(s[side, 8 * h:8 * h + 8] * w[j] for j, s in enumerate(stats))
            dst[256 + h:257 + h] = top[:1]
            dst[260 + h:261 + h] = jnp.sum(mass, axis=0, keepdims=True)
            parts = [a[side, h * HEAD:(h + 1) * HEAD].reshape(8, 8, 256) * w[j][None] for j, a in enumerate(accs)]
            dst[h * HEAD:(h + 1) * HEAD] = functools.reduce(jnp.add, parts).reshape(HEAD, 256)


def merge(info, parts):
    shape = jax.ShapeDtypeStruct((264, 256), f32)
    return pl.pallas_call(
        functools.partial(merge_kernel, count=len(parts)), out_shape=(shape, shape),
        in_specs=[scalars(), *vmem(2 * len(parts))], out_specs=tuple(vmem(2)),
        compiler_params=pltpu.CompilerParams(vmem_limit_bytes=16 * 1024 * 1024), name="merge",
    )(info, *[p[0] for p in parts], *[p[1] for p in parts])


def finish_kernel(keep, got, out):
    peak = jnp.maximum(keep[256:260], got[256:260])
    wa, wb = jnp.exp(keep[256:260] - peak), jnp.exp(got[256:260] - peak)
    mass = keep[260:264] * wa + got[260:264] * wb
    for h in range(4):
        s = slice(h * HEAD, (h + 1) * HEAD)
        out[s] = ((keep[s] * wa[h:h + 1] + got[s] * wb[h:h + 1]) / mass[h:h + 1]).astype(bf16)


def finish(keep, got):
    return pl.pallas_call(finish_kernel, out_shape=jax.ShapeDtypeStruct((256, 256), bf16), in_specs=vmem(2), out_specs=vmem(1)[0],
                          compiler_params=SMALL, name="finish")(keep, got)


SP = ("sp_0", "sp_1", "sp_2")
SP_TP = ("sp_0", "sp_1", "sp_2", "tp")


def ring(count, step):
    return [(i, (i + step) % count) for i in range(count)]


def sum_at_owner(value):
    pieces = value.reshape(4, value.shape[0] // 4, value.shape[1])
    arrived = lax.all_to_all(pieces, "tp", split_axis=0, concat_axis=0, tiled=True)
    return arrived.astype(f32).sum(axis=0)


def shards(tokens, w_query, w_key, w_value, w_gate, gate_bias, w_output):
    rows, cols = lax.axis_size("sp_0"), lax.axis_size("sp_1")
    chips = rows * cols
    core, col = lax.axis_index("sp_2"), lax.axis_index("sp_1")
    chip = lax.axis_index("sp_0") * cols + col
    other = chips - 1 - chip
    behind = (chip > other).astype(jnp.int32)
    low, high = jnp.minimum(chip, other), jnp.maximum(chip, other)
    bias8 = jnp.broadcast_to(jnp.tile(gate_bias, 2)[:, None], (8, 128))

    def scalar_row(*values):
        return jnp.stack([jnp.asarray(v, jnp.int32) for v in values])

    copies = jnp.broadcast_to(tokens, (4, *tokens.shape))
    here = lax.all_to_all(copies, "tp", split_axis=0, concat_axis=0, tiled=True)
    here = here.reshape(-1, tokens.shape[1])
    joined = jnp.concatenate([w_query, w_gate, w_key, w_value], axis=1)
    projected = lax.dot_general(joined, here, (((0,), (1,)), ((), ())), preferred_element_type=f32).astype(bf16)
    swapped = lax.ppermute(projected[:260], "sp_2", [(0, 1), (1, 0)])
    total, even, odd = sums(scalar_row(core), projected, swapped, bias8)
    far = [(2 * c + e, 2 * (chips - 1 - c) + e) for c in range(chips) for e in range(2)]
    crossed = lax.ppermute(odd, SP, far)
    row = lax.all_to_all(jnp.broadcast_to(total, (cols, *total.shape)), "sp_1", split_axis=0, concat_axis=0, tiled=True)
    payload = pack(projected, total, row)
    column = lax.all_to_all(jnp.broadcast_to(payload, (rows, *payload.shape)), "sp_0", split_axis=0, concat_axis=0, tiled=True)
    own, rhs = prepare(scalar_row(core, col, behind), column, even, crossed, bias8, cols)

    parts = []
    up, down = own, own
    pending, where = [own], [col]
    for step in range(1, cols // 2 + 1):
        up = lax.ppermute(up, "sp_1", ring(cols, 1))
        following, places = [up], [(col - step) % cols]
        if 2 * step < cols:
            down = lax.ppermute(down, "sp_1", ring(cols, -1))
            following.append(down)
            places.append((col + step) % cols)
        parts.append(attend(scalar_row(core, low, high, where[0], where[-1], behind), rhs, pending, cols))
        pending, where = following, places
    parts.append(attend(scalar_row(core, low, high, where[0], where[-1], behind), rhs, pending, cols))
    mine = jnp.where(behind == 1, 1 - core, core)
    keep, give = merge(scalar_row(mine, 1 - mine), parts)
    got = lax.ppermute(give, "sp_2", [(0, 1), (1, 0)])
    attended = finish(keep, got)
    back = [(2 * c + 1, 2 * (chips - 1 - c) + 1) for c in range(chips)]
    returned = lax.ppermute(attended, SP, back)
    attended = jnp.where(core == 0, attended, returned)
    partial = lax.dot_general(attended, w_output, (((0,), (0,)), ((), ())), preferred_element_type=f32).astype(bf16)
    return sum_at_owner(partial).astype(bf16)


def solution(mesh):
    finer = Mesh(mesh.devices.reshape(8, 8, 2, mesh.shape["tp"]), SP_TP)
    placed = (P(SP_TP, None), P(None, "tp"), P(None, "tp"), P(None, "tp"), P(None, "tp"), P("tp"), P("tp", None))

    return jax.shard_map(shards, mesh=finer, in_specs=placed, out_specs=P(SP_TP, None), check_vma=False)
```

```python
import functools
import jax, jax.numpy as jnp
from jax import lax
from jax.experimental import pallas as pl
from jax.experimental.pallas import tpu as pltpu
from jax.sharding import Mesh
from jax.sharding import PartitionSpec as P

f32, bf16 = jnp.float32, jnp.bfloat16
HEAD = 64
NEG = -1e30
LOW = -1e20
PIECES = 4
LOADAT = 3
SMALL = pltpu.CompilerParams(vmem_limit_bytes=8 * 1024 * 1024)


def split3(x):
    a = x.astype(bf16).astype(f32)
    r = x - a
    b = r.astype(bf16).astype(f32)
    return a, b, r - b


def log_sigmoid(u):
    x = jnp.exp(-jnp.abs(u))
    series = x * (1 - x * (1 / 2 - x * (1 / 3 - x * (1 / 4 - x * (1 / 5 - x * (1 / 6 - x * (1 / 7)))))))
    return jnp.minimum(u, 0.0) - jnp.where(x < 0.0625, series, jnp.log(1 + x))


def dot(a, b):
    return jnp.dot(a, b, preferred_element_type=f32)


def vmem(count):
    return [pl.BlockSpec(memory_space=pltpu.VMEM)] * count


def scalars():
    return pl.BlockSpec(memory_space=pltpu.SMEM)


def sums_kernel(info, mine, theirs, bias, total, even, odd):
    first = info[0] == 0
    own, other = mine[256:260].astype(f32), theirs[256:260].astype(f32)
    gates = jnp.concatenate([jnp.where(first, own, other), jnp.where(first, other, own)], axis=0)
    logs = jnp.sum(log_sigmoid(gates + bias[:, :1]), axis=1, keepdims=True)
    both = logs[:4] + logs[4:]
    total[...] = jnp.broadcast_to(jnp.concatenate([both, logs[:4]], axis=0), total.shape)

    @pl.when(first)
    def _():
        even[...] = mine[0:256]
        odd[...] = theirs[0:256]

    @pl.when(jnp.logical_not(first))
    def _():
        even[...] = theirs[0:256]
        odd[...] = mine[0:256]


def sums(info, mine, theirs, bias8):
    blk = mine.shape[1]
    half = jax.ShapeDtypeStruct((256, blk), bf16)
    return pl.pallas_call(
        sums_kernel, out_shape=(jax.ShapeDtypeStruct((8, 128), f32), half, half),
        in_specs=[scalars(), *vmem(3)], out_specs=tuple(vmem(3)), compiler_params=SMALL, name="sums",
    )(info, mine, theirs, bias8)


def pack_kernel(mine, total, row, payload, *, cols):
    payload[0:128] = mine[260:388]
    lane = lax.broadcasted_iota(jnp.int32, (4, 128), 1)
    held = jnp.zeros((4, 128), f32)
    for j in range(cols + 1):
        values = row[j, 0:4] if j < cols else total[4:8]
        for p, part in enumerate(split3(values)):
            held = jnp.where(lane == 16 * p + j, part, held)
    held = jnp.concatenate([held, jnp.zeros((4, 128), f32)], axis=1)
    payload[128:136] = jnp.concatenate([mine[256:260].astype(f32), held], axis=0).astype(bf16)


def pack(mine, total, row):
    blk = mine.shape[1]
    return pl.pallas_call(
        functools.partial(pack_kernel, cols=row.shape[0]), out_shape=jax.ShapeDtypeStruct((136, blk), bf16),
        in_specs=vmem(3), out_specs=vmem(1)[0], compiler_params=SMALL, name="pack",
    )(mine, total, row)


def prepare_kernel(info, column, even, crossed, bias, chunk, rhs, *, rows, cols, blk):
    core, col = info[0], info[3]
    last = column[:, 128:136, :].astype(f32)
    logs = log_sigmoid(last + bias[...][None, :, :1]).reshape(rows * 8, blk)
    tri = (lax.broadcasted_iota(jnp.int32, (blk, blk), 0) <= lax.broadcasted_iota(jnp.int32, (blk, blk), 1)).astype(bf16)
    inner = sum(dot(p.astype(bf16), tri) for p in split3(logs)).reshape(rows, 8, blk)
    lane = lax.broadcasted_iota(jnp.int32, (rows, 8, blk), 2)
    which = lane & 15
    used = lane < 48
    whole = jnp.sum(jnp.where(used & (which < cols), last, 0.0), axis=2, keepdims=True)
    early = jnp.sum(jnp.where(used & ((which < col) | ((which == cols) & (core == 1))), last, 0.0), axis=2, keepdims=True)
    before = jnp.zeros((4, 1), f32)
    for i in range(rows):
        own = inner[i, :4] + (before + early[i, 4:])
        before = before + whole[i, 4:]
        chunk[i, 64:80] = jnp.concatenate([*split3(-own), jnp.zeros((4, blk), f32)], axis=0).astype(bf16)
        chunk[i, 0:64] = column[i, 0:64, :]
        chunk[i, 80:144] = column[i, 64:128, :]
    row16 = lax.broadcasted_iota(jnp.int32, (16, blk), 0)
    swap = info[4] == 1
    for side in range(2):
        for h in range(4):
            s = slice(h * HEAD, (h + 1) * HEAD)
            a, b = even[s].astype(f32), crossed[s].astype(f32)
            q = jnp.where(swap, b, a) if side == 0 else jnp.where(swap, a, b)
            mark = jnp.where((row16 == 12) | ((row16 < 12) & ((row16 & 3) == h)), 1.0, 0.0)
            rhs[side * 4 + h] = jnp.concatenate([q * 0.125, mark, jnp.zeros((48, blk), f32)], axis=0).astype(bf16)


def prepare(info, column, even, crossed, bias8, cols):
    rows, _, blk = column.shape
    return pl.pallas_call(
        functools.partial(prepare_kernel, rows=rows, cols=cols, blk=blk),
        out_shape=(jax.ShapeDtypeStruct((rows, 144, blk), bf16), jax.ShapeDtypeStruct((8, 128, blk), bf16)),
        in_specs=[scalars(), *vmem(4)], out_specs=tuple(vmem(2)), compiler_params=pltpu.CompilerParams(vmem_limit_bytes=16 * 1024 * 1024), name="prepare",
    )(info, column, even, crossed, bias8)


def attend_kernel(*refs, steps_away, rows, cols, blk):
    count = len(steps_away)
    info, rhs = refs[:2]
    chunks = refs[2:2 + count]
    acc, stat = refs[2 + count:4 + count]
    keys, scores, tops = refs[4 + count:]
    core = info[0]
    size = blk // PIECES
    row16 = lax.broadcasted_iota(jnp.int32, (16, blk), 0)
    acc[...] = jnp.zeros_like(acc)
    for side in range(2):
        stat[side, 0:32] = jnp.zeros((32, blk), f32)
        stat[side, 32:64] = jnp.full((32, blk), LOW, f32)
    for n in range(count):
        kv = chunks[n]
        col = lax.rem(info[3] + (steps_away[n] + cols), cols)
        ahead = [jnp.clip((info[1 + side] - col + cols - 1) // cols, 0, rows) for side in range(2)]
        diag = [(info[1 + side] - col) % cols == 0 for side in range(2)]
        full = [jnp.where(diag[side], ahead[side], ahead[side] + 1) // 2 for side in range(2)]
        steps = full[0] + full[1]

        def place(it):
            side = (it >= full[0]).astype(jnp.int32)
            return side, jnp.clip(it - side * full[0], 0, rows // 2 - 1)

        def load_keys(slot, jj, count):
            for e in range(2):
                marks = kv[2 * jj + e, 64:80, :].astype(f32)
                marks = jnp.where((row16 == 12) & (2 * jj + e >= count), NEG, marks).astype(bf16)
                keys[slot, e * blk:(e + 1) * blk] = jnp.concatenate([kv[2 * jj + e, 0:64, :], marks, kv[2 * jj + e, 80:128, :]], axis=0).T

        def fused(nxt, cur, allowed=None):
            if cur is not None:
                slot, jj, side, h = cur
                old = stat[side, 32 + 8 * h:40 + 8 * h]
                new = jnp.maximum(old, jnp.max(tops[slot], axis=0, keepdims=True))
                scale = jnp.exp(old - new)
                mass = stat[side, 8 * h:8 * h + 8] * scale
                out = jnp.zeros((64, blk), f32)
            top = None
            for e in range(2):
                ps = []
                for g in range(PIECES):
                    at = e * blk + g * size
                    if nxt is not None:
                        s = dot(keys[nxt[1], at:at + size], rhs[nxt[2] * 4 + nxt[3]])
                        if allowed is not None:
                            s = jnp.where(allowed[at:at + size], s, NEG)
                        scores[nxt[0], at:at + size] = s
                        t = jnp.max(s.reshape(size // 8, 8, blk), axis=0)
                        top = t if top is None else jnp.maximum(top, t)
                    if cur is not None:
                        p = jnp.exp(scores[slot, at:at + size].reshape(size // 8, 8, blk) - new[None])
                        mass = mass + jnp.sum(p, axis=0)
                        ps.append(p.reshape(size, blk).astype(bf16))
                if cur is not None:
                    out = out + dot(kv[2 * jj + e, 80:144, :], jnp.concatenate(ps, axis=0))
            if nxt is not None:
                tops[nxt[0]] = top
            if cur is not None:
                stat[side, 8 * h:8 * h + 8] = mass
                stat[side, 32 + 8 * h:40 + 8 * h] = new
                a = acc[side, h * HEAD:(h + 1) * HEAD].reshape(8, 8, blk) * scale[None]
                acc[side, h * HEAD:(h + 1) * HEAD] = a.reshape(64, blk) + out

        @pl.when(steps > 0)
        def _():
            side, jj = place(0)
            load_keys(0, jj, jnp.where(side == 0, ahead[0], ahead[1]))
            fused((0, 0, side, 0), None)

            def body(it, carry):
                slot = it & 1
                side, jj = place(it)
                side_next, jj_next = place(jnp.minimum(it + 1, steps - 1))
                for h in range(4):
                    if h == LOADAT:
                        load_keys(1 - slot, jj_next, jnp.where(side_next == 0, ahead[0], ahead[1]))
                    nxt = ((h + 1) & 1, slot, side, h + 1) if h < 3 else (0, 1 - slot, side_next, 0)
                    fused(nxt, (h & 1, jj, side, h))
                return carry

            lax.fori_loop(0, steps, body, 0)

        def edge(side, carry):
            @pl.when(jnp.where(side == 0, diag[0], diag[1]))
            def _():
                chip = jnp.where(side == 0, info[1], info[2])
                jj = jnp.clip(jnp.where(side == 0, full[0], full[1]), 0, rows // 2 - 1)
                par = jnp.where(side == 0, info[4], 1 - info[4])
                qpos = (2 * chip + par) * blk + lax.broadcasted_iota(jnp.int32, (2 * blk, blk), 1)
                row = lax.broadcasted_iota(jnp.int32, (2 * blk, blk), 0)
                upper = (row >= blk).astype(jnp.int32)
                kpos = row + upper * ((2 * cols - 1) * blk) + ((2 * jj * cols + col) * 2 + core) * blk
                allowed = kpos <= qpos
                load_keys(0, jj, rows)
                fused((0, 0, side, 0), None, allowed)
                for h in range(4):
                    fused(((h + 1) & 1, 0, side, h + 1) if h < 3 else None, (h & 1, jj, side, h), allowed)

            return carry

        lax.fori_loop(0, 2, edge, 0)


def attend(info, rhs, chunks, steps_away, cols):
    rows, _, blk = chunks[0].shape
    return pl.pallas_call(
        functools.partial(attend_kernel, steps_away=steps_away, rows=rows, cols=cols, blk=blk),
        out_shape=(jax.ShapeDtypeStruct((2, 256, blk), f32), jax.ShapeDtypeStruct((2, 64, blk), f32)),
        in_specs=[scalars(), *vmem(1 + len(chunks))], out_specs=tuple(vmem(2)),
        scratch_shapes=[pltpu.VMEM((2, 2 * blk, 128), bf16), pltpu.VMEM((2, 2 * blk, blk), f32), pltpu.VMEM((2, 8, blk), f32)],
        compiler_params=pltpu.CompilerParams(vmem_limit_bytes=16 * 1024 * 1024), name="attend",
    )(info, rhs, *chunks)


def merge_kernel(*refs, count):
    info, accs, stats = refs[0], refs[1:1 + count], refs[1 + count:1 + 2 * count]
    keep, give = refs[1 + 2 * count:]
    for which in range(2):
        dst, side = (keep, give)[which], info[5] if which == 0 else 1 - info[5]
        for h in range(4):
            tops = [s[side, 32 + 8 * h:40 + 8 * h] for s in stats]
            top = functools.reduce(jnp.maximum, tops)
            w = [jnp.exp(t - top) for t in tops]
            mass = sum(s[side, 8 * h:8 * h + 8] * w[j] for j, s in enumerate(stats))
            dst[256 + h:257 + h] = top[:1]
            dst[260 + h:261 + h] = jnp.sum(mass, axis=0, keepdims=True)
            parts = [a[side, h * HEAD:(h + 1) * HEAD].reshape(8, 8, 256) * w[j][None] for j, a in enumerate(accs)]
            dst[h * HEAD:(h + 1) * HEAD] = functools.reduce(jnp.add, parts).reshape(HEAD, 256)


def merge(info, parts):
    shape = jax.ShapeDtypeStruct((264, 256), f32)
    return pl.pallas_call(
        functools.partial(merge_kernel, count=len(parts)), out_shape=(shape, shape),
        in_specs=[scalars(), *vmem(2 * len(parts))], out_specs=tuple(vmem(2)),
        compiler_params=pltpu.CompilerParams(vmem_limit_bytes=16 * 1024 * 1024), name="merge",
    )(info, *[p[0] for p in parts], *[p[1] for p in parts])


def finish_kernel(keep, got, out):
    peak = jnp.maximum(keep[256:260], got[256:260])
    wa, wb = jnp.exp(keep[256:260] - peak), jnp.exp(got[256:260] - peak)
    mass = keep[260:264] * wa + got[260:264] * wb
    heads = []
    for h in range(4):
        s = slice(h * HEAD, (h + 1) * HEAD)
        heads.append((keep[s] * wa[h:h + 1] + got[s] * wb[h:h + 1]) / mass[h:h + 1])
    out[...] = jnp.concatenate(heads, axis=0).T.astype(bf16)


def finish(keep, got):
    return pl.pallas_call(finish_kernel, out_shape=jax.ShapeDtypeStruct((256, 256), bf16), in_specs=vmem(2), out_specs=vmem(1)[0],
                          compiler_params=SMALL, name="finish")(keep, got)


def project_kernel(info, heads, *refs, shifts):
    weights, out = refs[:-1], refs[-1]
    total = None
    for k, shift in enumerate(shifts):
        part = dot(heads[lax.rem(info[6] + (4 - shift), 4)], weights[k][...]).astype(bf16).astype(f32)
        total = part if total is None else total + part
    out[...] = total.astype(bf16)


def project(info, heads, weights, shifts):
    shape = jax.ShapeDtypeStruct((heads.shape[1], weights[0].shape[1]), bf16)
    return pl.pallas_call(
        functools.partial(project_kernel, shifts=shifts), out_shape=shape, in_specs=[scalars(), *vmem(1 + len(weights))],
        out_specs=vmem(1)[0], compiler_params=pltpu.CompilerParams(vmem_limit_bytes=16 * 1024 * 1024), name="project",
    )(info, heads, *weights)


SP = ("sp_0", "sp_1", "sp_2")
SP_TP = ("sp_0", "sp_1", "sp_2", "tp")


def ring(count, step):
    return [(i, (i + step) % count) for i in range(count)]


def shards(tokens, w_query, w_key, w_value, w_gate, gate_bias, w_output):
    rows, cols = lax.axis_size("sp_0"), lax.axis_size("sp_1")
    chips = rows * cols
    core, col = lax.axis_index("sp_2"), lax.axis_index("sp_1")
    chip = lax.axis_index("sp_0") * cols + col
    other = chips - 1 - chip
    behind = (chip > other).astype(jnp.int32)
    low, high = jnp.minimum(chip, other), jnp.maximum(chip, other)
    mine = jnp.where(behind == 1, 1 - core, core)
    info = jnp.stack([jnp.asarray(v, jnp.int32) for v in (core, low, high, col, behind, mine, lax.axis_index("tp"))])
    bias8 = jnp.broadcast_to(jnp.tile(gate_bias, 2)[:, None], (8, 128))

    copies = jnp.broadcast_to(tokens, (4, *tokens.shape))
    here = lax.all_to_all(copies, "tp", split_axis=0, concat_axis=0, tiled=True)
    here = here.reshape(-1, tokens.shape[1])
    joined = jnp.concatenate([w_query, w_gate, w_key, w_value], axis=1)
    projected = lax.dot_general(joined, here, (((0,), (1,)), ((), ())), preferred_element_type=f32).astype(bf16)
    swapped = lax.ppermute(projected[:260], "sp_2", [(0, 1), (1, 0)])
    total, even, odd = sums(info, projected, swapped, bias8)
    far = [(2 * c + e, 2 * (chips - 1 - c) + e) for c in range(chips) for e in range(2)]
    crossed = lax.ppermute(odd, SP, far)
    row = lax.all_to_all(jnp.broadcast_to(total, (cols, *total.shape)), "sp_1", split_axis=0, concat_axis=0, tiled=True)
    payload = pack(projected, total, row)
    column = lax.all_to_all(jnp.broadcast_to(payload, (rows, *payload.shape)), "sp_0", split_axis=0, concat_axis=0, tiled=True)
    shifts, weights = (0, 1, 3, 2), [w_output]
    for shift in shifts[1:]:
        weights.append(lax.ppermute(w_output, "tp", ring(4, shift)))
    own, rhs = prepare(info, column, even, crossed, bias8, cols)

    parts = []
    up, down = own, own
    pending, where = [own], (0,)
    for step in range(1, cols // 2 + 1):
        up = lax.ppermute(up, "sp_1", ring(cols, 1))
        following, places = [up], (-step,)
        if 2 * step < cols:
            down = lax.ppermute(down, "sp_1", ring(cols, -1))
            following.append(down)
            places = (-step, step)
        parts.append(attend(info, rhs, pending, where, cols))
        pending, where = following, places
    parts.append(attend(info, rhs, pending, where, cols))
    keep, give = merge(info, parts)
    got = lax.ppermute(give, "sp_2", [(0, 1), (1, 0)])
    attended = finish(keep, got)
    back = [(2 * c + 1, 2 * (chips - 1 - c) + 1) for c in range(chips)]
    returned = lax.ppermute(attended, SP, back)
    attended = jnp.where(core == 0, attended, returned)
    heads = lax.all_to_all(attended.reshape(4, -1, attended.shape[1]), "tp", split_axis=0, concat_axis=0, tiled=True)
    return project(info, heads, weights, shifts)


def solution(mesh):
    finer = Mesh(mesh.devices.reshape(8, 8, 2, mesh.shape["tp"]), SP_TP)
    placed = (P(SP_TP, None), P(None, "tp"), P(None, "tp"), P(None, "tp"), P(None, "tp"), P("tp"), P("tp", None))

    return jax.shard_map(shards, mesh=finer, in_specs=placed, out_specs=P(SP_TP, None), check_vma=False)
```

```python
import functools
import jax, jax.numpy as jnp
from jax import lax
from jax.experimental import pallas as pl
from jax.experimental.pallas import tpu as pltpu
from jax.sharding import Mesh
from jax.sharding import PartitionSpec as P

f32, bf16 = jnp.float32, jnp.bfloat16
HEAD = 64
NEG = -1e30
LOW = -1e20
PIECES = 4
LOADAT = 3
SMALL = pltpu.CompilerParams(vmem_limit_bytes=8 * 1024 * 1024)


def split3(x):
    a = x.astype(bf16).astype(f32)
    r = x - a
    b = r.astype(bf16).astype(f32)
    return a, b, r - b


def log_sigmoid(u):
    x = jnp.exp(-jnp.abs(u))
    series = x * (1 - x * (1 / 2 - x * (1 / 3 - x * (1 / 4 - x * (1 / 5 - x * (1 / 6 - x * (1 / 7)))))))
    return jnp.minimum(u, 0.0) - jnp.where(x < 0.0625, series, jnp.log(1 + x))


def dot(a, b):
    return jnp.dot(a, b, preferred_element_type=f32)


def vmem(count):
    return [pl.BlockSpec(memory_space=pltpu.VMEM)] * count


def scalars():
    return pl.BlockSpec(memory_space=pltpu.SMEM)


def sums_kernel(info, mine, theirs, bias, total, even, odd):
    first = info[0] == 0
    own, other = mine[256:260].astype(f32), theirs[256:260].astype(f32)
    gates = jnp.concatenate([jnp.where(first, own, other), jnp.where(first, other, own)], axis=0)
    logs = jnp.sum(log_sigmoid(gates + bias[:, :1]), axis=1, keepdims=True)
    both = logs[:4] + logs[4:]
    total[...] = jnp.broadcast_to(jnp.concatenate([both, logs[:4]], axis=0), total.shape)

    @pl.when(first)
    def _():
        even[...] = mine[0:256]
        odd[...] = theirs[0:256]

    @pl.when(jnp.logical_not(first))
    def _():
        even[...] = theirs[0:256]
        odd[...] = mine[0:256]


def sums(info, mine, theirs, bias8):
    blk = mine.shape[1]
    half = jax.ShapeDtypeStruct((256, blk), bf16)
    return pl.pallas_call(
        sums_kernel, out_shape=(jax.ShapeDtypeStruct((8, 128), f32), half, half),
        in_specs=[scalars(), *vmem(3)], out_specs=tuple(vmem(3)), compiler_params=SMALL, name="sums",
    )(info, mine, theirs, bias8)


def pack_kernel(mine, total, row, payload, *, cols):
    payload[0:128] = mine[260:388]
    lane = lax.broadcasted_iota(jnp.int32, (4, 128), 1)
    held = jnp.zeros((4, 128), f32)
    for j in range(cols + 1):
        values = row[j, 0:4] if j < cols else total[4:8]
        for p, part in enumerate(split3(values)):
            held = jnp.where(lane == 16 * p + j, part, held)
    held = jnp.concatenate([held, jnp.zeros((4, 128), f32)], axis=1)
    payload[128:136] = jnp.concatenate([mine[256:260].astype(f32), held], axis=0).astype(bf16)


def pack(mine, total, row):
    blk = mine.shape[1]
    return pl.pallas_call(
        functools.partial(pack_kernel, cols=row.shape[0]), out_shape=jax.ShapeDtypeStruct((136, blk), bf16),
        in_specs=vmem(3), out_specs=vmem(1)[0], compiler_params=SMALL, name="pack",
    )(mine, total, row)


def prepare_kernel(info, column, even, crossed, bias, chunk, rhs, *, rows, cols, blk):
    core, col = info[0], info[3]
    last = column[:, 128:136, :].astype(f32)
    logs = log_sigmoid(last + bias[...][None, :, :1]).reshape(rows * 8, blk)
    tri = (lax.broadcasted_iota(jnp.int32, (blk, blk), 0) <= lax.broadcasted_iota(jnp.int32, (blk, blk), 1)).astype(bf16)
    inner = sum(dot(p.astype(bf16), tri) for p in split3(logs)).reshape(rows, 8, blk)
    lane = lax.broadcasted_iota(jnp.int32, (rows, 8, blk), 2)
    which = lane & 15
    used = lane < 48
    whole = jnp.sum(jnp.where(used & (which < cols), last, 0.0), axis=2, keepdims=True)
    early = jnp.sum(jnp.where(used & ((which < col) | ((which == cols) & (core == 1))), last, 0.0), axis=2, keepdims=True)
    before = jnp.zeros((4, 1), f32)
    for i in range(rows):
        own = inner[i, :4] + (before + early[i, 4:])
        before = before + whole[i, 4:]
        chunk[i, 64:80] = jnp.concatenate([*split3(-own), jnp.zeros((4, blk), f32)], axis=0).astype(bf16)
        chunk[i, 0:64] = column[i, 0:64, :]
        chunk[i, 80:144] = column[i, 64:128, :]
    row16 = lax.broadcasted_iota(jnp.int32, (16, blk), 0)
    swap = info[4] == 1
    for side in range(2):
        for h in range(4):
            s = slice(h * HEAD, (h + 1) * HEAD)
            a, b = even[s].astype(f32), crossed[s].astype(f32)
            q = jnp.where(swap, b, a) if side == 0 else jnp.where(swap, a, b)
            mark = jnp.where((row16 == 12) | ((row16 < 12) & ((row16 & 3) == h)), 1.0, 0.0)
            rhs[side * 4 + h] = jnp.concatenate([q * 0.125, mark, jnp.zeros((48, blk), f32)], axis=0).astype(bf16)


def prepare(info, column, even, crossed, bias8, cols):
    rows, _, blk = column.shape
    return pl.pallas_call(
        functools.partial(prepare_kernel, rows=rows, cols=cols, blk=blk),
        out_shape=(jax.ShapeDtypeStruct((rows, 144, blk), bf16), jax.ShapeDtypeStruct((8, 128, blk), bf16)),
        in_specs=[scalars(), *vmem(4)], out_specs=tuple(vmem(2)), compiler_params=pltpu.CompilerParams(vmem_limit_bytes=16 * 1024 * 1024), name="prepare",
    )(info, column, even, crossed, bias8)


def attend_kernel(*refs, steps_away, rows, cols, blk):
    count = len(steps_away)
    info, rhs = refs[:2]
    chunks = refs[2:2 + count]
    acc, stat = refs[2 + count:4 + count]
    keys, scores, tops = refs[4 + count:]
    core = info[0]
    size = blk // PIECES
    row16 = lax.broadcasted_iota(jnp.int32, (16, blk), 0)
    acc[...] = jnp.zeros_like(acc)
    for side in range(2):
        stat[side, 0:32] = jnp.zeros((32, blk), f32)
        stat[side, 32:64] = jnp.full((32, blk), LOW, f32)
    columns = [lax.rem(info[3] + (away + cols), cols) for away in steps_away]
    ahead = [[jnp.clip((info[1 + side] - col + cols - 1) // cols, 0, rows) for col in columns] for side in range(2)]
    own = [[(info[1 + side] - col) % cols == 0 for col in columns] for side in range(2)]
    if count == 2:
        tiles = rows
        diag = [o[0] | o[1] for o in own]
        full = [jnp.where(o[0], x[0], jnp.where(o[1], x[1], jnp.maximum(x[0], x[1]))) for o, x in zip(own, ahead)]
    else:
        tiles = rows // 2
        diag = [o[0] for o in own]
        full = [jnp.where(o[0], x[0], x[0] + 1) // 2 for o, x in zip(own, ahead)]
    steps = full[0] + full[1]

    def half(jj, e):
        return (e, jj) if count == 2 else (0, 2 * jj + e)

    def limits(side):
        return [jnp.where(side == 0, ahead[0][n], ahead[1][n]) for n in range(count)]

    def place(it):
        side = (it >= full[0]).astype(jnp.int32)
        return side, jnp.clip(it - side * full[0], 0, tiles - 1)

    def load_keys(slot, jj, counts):
        for e in range(2):
            n, j = half(jj, e)
            kv = chunks[n]
            marks = kv[j, 64:80, :].astype(f32)
            marks = jnp.where((row16 == 12) & (j >= counts[n]), NEG, marks).astype(bf16)
            keys[slot, e * blk:(e + 1) * blk] = jnp.concatenate([kv[j, 0:64, :], marks, kv[j, 80:128, :]], axis=0).T

    def fused(nxt, cur, allowed=None):
        if cur is not None:
            slot, jj, side, h = cur
            old = stat[side, 32 + 8 * h:40 + 8 * h]
            new = jnp.maximum(old, jnp.max(tops[slot], axis=0, keepdims=True))
            scale = jnp.exp(old - new)
            mass = stat[side, 8 * h:8 * h + 8] * scale
            out = jnp.zeros((64, blk), f32)
        top = None
        for e in range(2):
            ps = []
            for g in range(PIECES):
                at = e * blk + g * size
                if nxt is not None:
                    s = dot(keys[nxt[1], at:at + size], rhs[nxt[2] * 4 + nxt[3]])
                    if allowed is not None:
                        s = jnp.where(allowed[at:at + size], s, NEG)
                    scores[nxt[0], at:at + size] = s
                    t = jnp.max(s.reshape(size // 8, 8, blk), axis=0)
                    top = t if top is None else jnp.maximum(top, t)
                if cur is not None:
                    p = jnp.exp(scores[slot, at:at + size].reshape(size // 8, 8, blk) - new[None])
                    mass = mass + jnp.sum(p, axis=0)
                    ps.append(p.reshape(size, blk).astype(bf16))
            if cur is not None:
                n, j = half(jj, e)
                out = out + dot(chunks[n][j, 80:144, :], jnp.concatenate(ps, axis=0))
        if nxt is not None:
            tops[nxt[0]] = top
        if cur is not None:
            stat[side, 8 * h:8 * h + 8] = mass
            stat[side, 32 + 8 * h:40 + 8 * h] = new
            a = acc[side, h * HEAD:(h + 1) * HEAD].reshape(8, 8, blk) * scale[None]
            acc[side, h * HEAD:(h + 1) * HEAD] = a.reshape(64, blk) + out

    @pl.when(steps > 0)
    def _():
        side, jj = place(0)
        load_keys(0, jj, limits(side))
        fused((0, 0, side, 0), None)

        def body(it, carry):
            slot = it & 1
            side, jj = place(it)
            side_next, jj_next = place(jnp.minimum(it + 1, steps - 1))
            for h in range(4):
                if h == LOADAT:
                    load_keys(1 - slot, jj_next, limits(side_next))
                nxt = ((h + 1) & 1, slot, side, h + 1) if h < 3 else (0, 1 - slot, side_next, 0)
                fused(nxt, (h & 1, jj, side, h))
            return carry

        lax.fori_loop(0, steps, body, 0)

    def edge(side, carry):
        @pl.when(jnp.where(side == 0, diag[0], diag[1]))
        def _():
            chip = jnp.where(side == 0, info[1], info[2])
            jj = jnp.clip(jnp.where(side == 0, full[0], full[1]), 0, tiles - 1)
            par = jnp.where(side == 0, info[4], 1 - info[4])
            qpos = (2 * chip + par) * blk + lax.broadcasted_iota(jnp.int32, (2 * blk, blk), 1)
            row = lax.broadcasted_iota(jnp.int32, (2 * blk, blk), 0)
            starts = []
            for e in range(2):
                n, j = half(jj, e)
                starts.append((2 * (j * cols + columns[n]) + core - e) * blk)
            kpos = row + jnp.where(row >= blk, starts[1], starts[0])
            allowed = kpos <= qpos
            load_keys(0, jj, [rows] * count)
            fused((0, 0, side, 0), None, allowed)
            for h in range(4):
                fused(((h + 1) & 1, 0, side, h + 1) if h < 3 else None, (h & 1, jj, side, h), allowed)

        return carry

    lax.fori_loop(0, 2, edge, 0)


def attend(info, rhs, chunks, steps_away, cols):
    rows, _, blk = chunks[0].shape
    return pl.pallas_call(
        functools.partial(attend_kernel, steps_away=steps_away, rows=rows, cols=cols, blk=blk),
        out_shape=(jax.ShapeDtypeStruct((2, 256, blk), f32), jax.ShapeDtypeStruct((2, 64, blk), f32)),
        in_specs=[scalars(), *vmem(1 + len(chunks))], out_specs=tuple(vmem(2)),
        scratch_shapes=[pltpu.VMEM((2, 2 * blk, 128), bf16), pltpu.VMEM((2, 2 * blk, blk), f32), pltpu.VMEM((2, 8, blk), f32)],
        compiler_params=pltpu.CompilerParams(vmem_limit_bytes=16 * 1024 * 1024), name="attend",
    )(info, rhs, *chunks)


def merge_kernel(*refs, count):
    info, accs, stats = refs[0], refs[1:1 + count], refs[1 + count:1 + 2 * count]
    keep, give = refs[1 + 2 * count:]
    for which in range(2):
        dst, side = (keep, give)[which], info[5] if which == 0 else 1 - info[5]
        for h in range(4):
            tops = [s[side, 32 + 8 * h:40 + 8 * h] for s in stats]
            top = functools.reduce(jnp.maximum, tops)
            w = [jnp.exp(t - top) for t in tops]
            mass = sum(s[side, 8 * h:8 * h + 8] * w[j] for j, s in enumerate(stats))
            dst[256 + h:257 + h] = top[:1]
            dst[260 + h:261 + h] = jnp.sum(mass, axis=0, keepdims=True)
            parts = [a[side, h * HEAD:(h + 1) * HEAD].reshape(8, 8, 256) * w[j][None] for j, a in enumerate(accs)]
            dst[h * HEAD:(h + 1) * HEAD] = functools.reduce(jnp.add, parts).reshape(HEAD, 256)


def merge(info, parts):
    shape = jax.ShapeDtypeStruct((264, 256), f32)
    return pl.pallas_call(
        functools.partial(merge_kernel, count=len(parts)), out_shape=(shape, shape),
        in_specs=[scalars(), *vmem(2 * len(parts))], out_specs=tuple(vmem(2)),
        compiler_params=pltpu.CompilerParams(vmem_limit_bytes=16 * 1024 * 1024), name="merge",
    )(info, *[p[0] for p in parts], *[p[1] for p in parts])


def finish_kernel(keep, got, out):
    peak = jnp.maximum(keep[256:260], got[256:260])
    wa, wb = jnp.exp(keep[256:260] - peak), jnp.exp(got[256:260] - peak)
    mass = keep[260:264] * wa + got[260:264] * wb
    heads = []
    for h in range(4):
        s = slice(h * HEAD, (h + 1) * HEAD)
        heads.append((keep[s] * wa[h:h + 1] + got[s] * wb[h:h + 1]) / mass[h:h + 1])
    out[...] = jnp.concatenate(heads, axis=0).T.astype(bf16)


def finish(keep, got):
    return pl.pallas_call(finish_kernel, out_shape=jax.ShapeDtypeStruct((256, 256), bf16), in_specs=vmem(2), out_specs=vmem(1)[0],
                          compiler_params=SMALL, name="finish")(keep, got)


def project_kernel(info, heads, *refs, shifts):
    weights, out = refs[:-1], refs[-1]
    total = None
    for k, shift in enumerate(shifts):
        part = dot(heads[lax.rem(info[6] + (4 - shift), 4)], weights[k][...]).astype(bf16).astype(f32)
        total = part if total is None else total + part
    out[...] = total.astype(bf16)


def project(info, heads, weights, shifts):
    shape = jax.ShapeDtypeStruct((heads.shape[1], weights[0].shape[1]), bf16)
    return pl.pallas_call(
        functools.partial(project_kernel, shifts=shifts), out_shape=shape, in_specs=[scalars(), *vmem(1 + len(weights))],
        out_specs=vmem(1)[0], compiler_params=pltpu.CompilerParams(vmem_limit_bytes=16 * 1024 * 1024), name="project",
    )(info, heads, *weights)


SP = ("sp_0", "sp_1", "sp_2")
SP_TP = ("sp_0", "sp_1", "sp_2", "tp")


def ring(count, step):
    return [(i, (i + step) % count) for i in range(count)]


def shards(tokens, w_query, w_key, w_value, w_gate, gate_bias, w_output):
    rows, cols = lax.axis_size("sp_0"), lax.axis_size("sp_1")
    chips = rows * cols
    core, col = lax.axis_index("sp_2"), lax.axis_index("sp_1")
    chip = lax.axis_index("sp_0") * cols + col
    other = chips - 1 - chip
    behind = (chip > other).astype(jnp.int32)
    low, high = jnp.minimum(chip, other), jnp.maximum(chip, other)
    mine = jnp.where(behind == 1, 1 - core, core)
    info = jnp.stack([jnp.asarray(v, jnp.int32) for v in (core, low, high, col, behind, mine, lax.axis_index("tp"))])
    bias8 = jnp.broadcast_to(jnp.tile(gate_bias, 2)[:, None], (8, 128))

    copies = jnp.broadcast_to(tokens, (4, *tokens.shape))
    here = lax.all_to_all(copies, "tp", split_axis=0, concat_axis=0, tiled=True)
    here = here.reshape(-1, tokens.shape[1])
    joined = jnp.concatenate([w_query, w_gate, w_key, w_value], axis=1)
    projected = lax.dot_general(joined, here, (((0,), (1,)), ((), ())), preferred_element_type=f32).astype(bf16)
    swapped = lax.ppermute(projected[:260], "sp_2", [(0, 1), (1, 0)])
    total, even, odd = sums(info, projected, swapped, bias8)
    far = [(2 * c + e, 2 * (chips - 1 - c) + e) for c in range(chips) for e in range(2)]
    crossed = lax.ppermute(odd, SP, far)
    row = lax.all_to_all(jnp.broadcast_to(total, (cols, *total.shape)), "sp_1", split_axis=0, concat_axis=0, tiled=True)
    payload = pack(projected, total, row)
    column = lax.all_to_all(jnp.broadcast_to(payload, (rows, *payload.shape)), "sp_0", split_axis=0, concat_axis=0, tiled=True)
    shifts, weights = (0, 1, 3, 2), [w_output]
    for shift in shifts[1:]:
        weights.append(lax.ppermute(w_output, "tp", ring(4, shift)))
    own, rhs = prepare(info, column, even, crossed, bias8, cols)

    parts = []
    up, down = own, own
    pending, where = [own], (0,)
    for step in range(1, cols // 2 + 1):
        up = lax.ppermute(up, "sp_1", ring(cols, 1))
        following, places = [up], (-step,)
        if 2 * step < cols:
            down = lax.ppermute(down, "sp_1", ring(cols, -1))
            following.append(down)
            places = (-step, step)
        parts.append(attend(info, rhs, pending, where, cols))
        pending, where = following, places
    parts.append(attend(info, rhs, pending, where, cols))
    keep, give = merge(info, parts)
    got = lax.ppermute(give, "sp_2", [(0, 1), (1, 0)])
    attended = finish(keep, got)
    back = [(2 * c + 1, 2 * (chips - 1 - c) + 1) for c in range(chips)]
    returned = lax.ppermute(attended, SP, back)
    attended = jnp.where(core == 0, attended, returned)
    heads = lax.all_to_all(attended.reshape(4, -1, attended.shape[1]), "tp", split_axis=0, concat_axis=0, tiled=True)
    return project(info, heads, weights, shifts)


def solution(mesh):
    finer = Mesh(mesh.devices.reshape(8, 8, 2, mesh.shape["tp"]), SP_TP)
    placed = (P(SP_TP, None), P(None, "tp"), P(None, "tp"), P(None, "tp"), P(None, "tp"), P("tp"), P("tp", None))

    return jax.shard_map(shards, mesh=finer, in_specs=placed, out_specs=P(SP_TP, None), check_vma=False)
```
